32 devices in a mesh: fs: 8 (over z, y), tp: 4 (over x, core).
Axes of the slice: x: 2, y: 2, z: 4, core: 2. Of those that a mesh axis runs over, the one named last changes fastest.
Arguments:
- tokens: bfloat16 [8192, 2048], P('fs'), may hold values from -6 to 6
- w_gate_side: bfloat16 [2048, 1024], P('fs', 'tp'), may hold values from -0.125 to 0.125
- w_value_side: bfloat16 [2048, 1024], P('fs', 'tp'), may hold values from -0.125 to 0.125
- spatial_gain: float32 [1024], P('tp'), may hold values from 0.1 to 1.9
- w_spatial: bfloat16 [16, 128, 128], P('tp'), may hold values from -0.5 to 0.5
- spatial_bias: float32 [16, 128], P('tp'), may hold values from 0.1 to 1.9
- w_mixer_out: bfloat16 [1024, 2048], P('tp', 'fs'), may hold values from -0.1875 to 0.1875
- first_gain: float32 [2048], replicated, may hold values from 0.1 to 1.9
- w_ff_gate: bfloat16 [2048, 5632], P('fs', 'tp'), may hold values from -0.125 to 0.125
- w_ff_up: bfloat16 [2048, 5632], P('fs', 'tp'), may hold values from -0.125 to 0.125
- conv_gate_taps: float32 [3, 5632], P(None, 'tp'), may hold values from -3.5 to 3.5
- conv_up_taps: float32 [3, 5632], P(None, 'tp'), may hold values from -3.5 to 3.5
- w_ff_down: bfloat16 [5632, 2048], P('tp', 'fs'), may hold values from -0.078125 to 0.078125
- second_gain: float32 [2048], replicated, may hold values from 0.1 to 1.9
Outputs:
- layer_out: bfloat16 [8192, 2048], P('fs', 'tp')
The draws below stay inside these ranges and needn't reach their ends.
All inputs are finite; a program needn't handle non-finite values.
Results may differ from the reference program's by a relative error of at most 0.015.
Values may be sent and summed in bfloat16 or wider, within the bound.
A program may use at most 64 MiB of HBM per device.

```python
import jax
import jax.numpy as jnp
from jax import lax

D = 2048
GROUPS = 16
GROUP_DIM = 64
SG_WIDTH = 1024
FF = 5632
SPAN = 128
SEQ = 256
TOKENS = 8192
N_TP = 4


def steps_of(stream_key, shape, split, least, high):
    def one(axis_at, blocks):
        steps = jax.random.uniform(jax.random.fold_in(jax.random.fold_in(stream_key, 6), axis_at), (blocks,), jnp.float32, least / len(split), high / len(split))
        return jnp.repeat(jnp.exp(steps), shape[axis_at] // blocks).reshape((-1,) + (1,) * (len(shape) - axis_at - 1))

    level = one(*split[0])
    for cut in split[1:]:
        level = level * one(*cut)
    return level


def noise(key, shape, scale, limit, shards=(), kind=jnp.bfloat16):
    level = steps_of(key, shape, shards, -0.22, 0.18) if shards else 1.0
    values = jax.random.normal(key, shape, jnp.float32) * scale * level
    return jnp.minimum(jnp.maximum(values, -limit), limit).astype(kind)


def setup_inputs(seed: int = 0) -> dict:
    key_of = jax.random.split(jax.random.key(seed), 15)
    tokens = noise(key_of[0], (TOKENS, D), 1.0, 6.0, ((0, 8),))
    w_gate_side = noise(key_of[1], (D, SG_WIDTH), D ** -0.5, 0.125, ((0, 8), (1, 4)))
    w_value_side = noise(key_of[2], (D, SG_WIDTH), D ** -0.5, 0.125, ((0, 8), (1, 4)))
    spatial_gain = jnp.clip(1.0 + 0.18 * jax.random.normal(key_of[3], (SG_WIDTH,), jnp.float32), 0.1, 1.9)
    w_spatial = noise(key_of[4], (GROUPS, SPAN, SPAN), SPAN ** -0.5, 0.5, ((0, 4),))
    spatial_bias = jnp.clip(1.0 + 0.18 * jax.random.normal(key_of[5], (GROUPS, SPAN), jnp.float32), 0.1, 1.9)
    w_mixer_out = noise(key_of[6], (SG_WIDTH, D), SG_WIDTH ** -0.5, 0.1875, ((0, 4), (1, 8)))
    first_gain = jnp.clip(1.0 + 0.18 * jax.random.normal(key_of[7], (D,), jnp.float32), 0.1, 1.9)
    w_ff_gate = noise(key_of[8], (D, FF), D ** -0.5, 0.125, ((0, 8), (1, 4)))
    w_ff_up = noise(key_of[9], (D, FF), D ** -0.5, 0.125, ((0, 8), (1, 4)))
    conv_gate_taps = noise(key_of[10], (3, FF), 3 ** -0.5, 3.5, ((1, 4),), jnp.float32)
    conv_up_taps = noise(key_of[11], (3, FF), 3 ** -0.5, 3.5, ((1, 4),), jnp.float32)
    w_ff_down = noise(key_of[12], (FF, D), FF ** -0.5, 0.078125, ((0, 4), (1, 8)))
    second_gain = jnp.clip(1.0 + 0.18 * jax.random.normal(key_of[13], (D,), jnp.float32), 0.1, 1.9)
    return {"tokens": tokens, "w_gate_side": w_gate_side, "w_value_side": w_value_side, "spatial_gain": spatial_gain, "w_spatial": w_spatial, "spatial_bias": spatial_bias, "w_mixer_out": w_mixer_out, "first_gain": first_gain, "w_ff_gate": w_ff_gate, "w_ff_up": w_ff_up, "conv_gate_taps": conv_gate_taps, "conv_up_taps": conv_up_taps, "w_ff_down": w_ff_down, "second_gain": second_gain}


residual_scale = 2.0 ** 0.25
norm_eps = 1e-05

def row_norm(values, gain):
    width = values.shape[-1]
    mean = lax.optimization_barrier(jnp.sum(values, axis=-1, keepdims=True)) / width
    square = lax.optimization_barrier(jnp.sum(values * values, axis=-1, keepdims=True)) / width
    spread = square - mean * mean
    return (values - mean) * lax.rsqrt(spread + norm_eps) * gain

def causal_taps(pre, taps):
    count = pre.shape[0] // SEQ
    blocks = pre.reshape(count, SEQ, pre.shape[1])
    padded = jnp.pad(blocks, ((0, 0), (2, 0), (0, 0)))
    result = padded[:, 0:SEQ] * taps[0] + padded[:, 1:SEQ + 1] * taps[1] + padded[:, 2:] * taps[2]
    return result.reshape(pre.shape)

def range_sum(left, right, parts):
    width = left.shape[1] // parts
    total = jnp.zeros((left.shape[0], right.shape[1]), jnp.float32)
    for index in range(parts):
        term = jnp.dot(left[:, index * width:(index + 1) * width], right[index * width:(index + 1) * width], preferred_element_type=jnp.float32)
        total = total + term.astype(jnp.bfloat16).astype(jnp.float32)
    return total

def reference(tokens, w_gate_side, w_value_side, spatial_gain, w_spatial, spatial_bias, w_mixer_out, first_gain, w_ff_gate, w_ff_up, conv_gate_taps, conv_up_taps, w_ff_down, second_gain):
    gate_act = jax.nn.gelu(jnp.dot(tokens, w_gate_side, preferred_element_type=jnp.float32))
    value_act = jax.nn.gelu(jnp.dot(tokens, w_value_side, preferred_element_type=jnp.float32))
    value_norm = row_norm(value_act, spatial_gain).astype(jnp.bfloat16)
    blocks = value_norm.reshape(TOKENS // SPAN, SPAN, GROUPS, GROUP_DIM).astype(jnp.float32)
    lower = jnp.tril(jnp.ones((SPAN, SPAN), jnp.float32))
    causal_w = w_spatial.astype(jnp.float32) * lower
    mixed = jnp.einsum('gts,nsgc->ntgc', causal_w, blocks) + spatial_bias.T[None, :, :, None]
    spatial_out = (gate_act * mixed.reshape(TOKENS, SG_WIDTH)).astype(jnp.bfloat16)
    mixer_sum = range_sum(spatial_out, w_mixer_out, N_TP)
    first_normed = row_norm(residual_scale * tokens.astype(jnp.float32) + mixer_sum, first_gain).astype(jnp.bfloat16)
    ff_gate = causal_taps(jnp.dot(first_normed, w_ff_gate, preferred_element_type=jnp.float32), conv_gate_taps)
    ff_up = causal_taps(jnp.dot(first_normed, w_ff_up, preferred_element_type=jnp.float32), conv_up_taps)
    ff_hidden = (jax.nn.silu(ff_gate) * ff_up).astype(jnp.bfloat16)
    ff_sum = range_sum(ff_hidden, w_ff_down, N_TP)
    layer_out = row_norm(residual_scale * first_normed.astype(jnp.float32) + ff_sum, second_gain)
    return layer_out.astype(jnp.bfloat16)
```

```python
import jax
import jax.numpy as jnp
from jax import lax
from jax.experimental import pallas as pl
from jax.experimental.pallas import tpu as pltpu
from jax.sharding import PartitionSpec as P

GROUP_DIM = 64
SPAN = 128
SEQ = 256
Z = 4
CORES = 2

residual_scale = 2.0**0.25
norm_eps = 1e-05


def fs_pairs(n_fs, dz, dy):
    n_y = n_fs // Z
    pairs = []
    for index in range(n_fs):
        z, y = index // n_y, index % n_y
        pairs.append((index, (z + dz) % Z * n_y + (y + dy) % n_y))
    return pairs


def tp_pairs(n_tp, dx, dc):
    n_x = n_tp // CORES
    pairs = []
    for index in range(n_tp):
        x, c = index // CORES, index % CORES
        pairs.append((index, (x + dx) % n_x * CORES + (c + dc) % CORES))
    return pairs


def move_fs(value, dz, dy):
    return lax.ppermute(value, "fs", fs_pairs(lax.axis_size("fs"), dz, dy))


def move_tp(value, dx, dc):
    return lax.ppermute(value, "tp", tp_pairs(lax.axis_size("tp"), dx, dc))


def y_blocks(own):
    n_y = lax.axis_size("fs") // Z
    y = lax.axis_index("fs") % n_y
    pieces = [own]
    for step in range(1, n_y):
        pieces.append(move_fs(pieces[-1], 0, 1))
    return [lax.select_n((y - at) % n_y, *pieces) if n_y > 2 else lax.select_n((y - at) % n_y == 1, *pieces) for at in range(n_y)]


def z_ring(own):
    right = move_fs(own, 1, 0)
    left = move_fs(own, -1, 0)
    far = move_fs(right, 1, 0)
    return [own, left, far, right]


def row_norm(values, gain):
    width = values.shape[1]
    mean = jnp.sum(values, axis=1, keepdims=True) / width
    spread = jnp.sum(values * values, axis=1, keepdims=True) / width - mean * mean
    return (values - mean) * lax.rsqrt(spread + norm_eps) * gain


def scatter_rows(part):
    n_tp = lax.axis_size("tp")
    n_x = n_tp // CORES
    tp = lax.axis_index("tp")
    x, c = tp // CORES, tp % CORES
    rows, cols = part.shape
    blocks = part.astype(jnp.bfloat16).reshape(n_x, CORES, rows // n_tp, cols)
    mine = lax.dynamic_index_in_dim(blocks, c, 1, keepdims=False)
    other = lax.dynamic_index_in_dim(blocks, 1 - c, 1, keepdims=False)
    pair = mine.astype(jnp.float32) + move_tp(other, 0, 1).astype(jnp.float32)
    total = lax.dynamic_index_in_dim(pair, x, 0, keepdims=False)
    for dx in range(1, n_x):
        away = lax.dynamic_index_in_dim(pair, (x + dx) % n_x, 0, keepdims=False)
        total = total + move_tp(away.astype(jnp.bfloat16), dx, 0).astype(jnp.float32)
    return total


def gather_rows(own):
    n_tp = lax.axis_size("tp")
    n_x = n_tp // CORES
    tp = lax.axis_index("tp")
    x, c = tp // CORES, tp % CORES
    column = [own]
    for dx in range(1, n_x):
        column.append(move_tp(own, dx, 0))
    column_abs = [
        lax.select_n((x - at) % n_x == 1, *column) if n_x == 2 else lax.select_n((x - at) % n_x, *column)
        for at in range(n_x)
    ]
    near = [move_tp(value, 0, 1) for value in column]
    near_abs = [
        lax.select_n((x - at) % n_x == 1, *near) if n_x == 2 else lax.select_n((x - at) % n_x, *near)
        for at in range(n_x)
    ]
    pieces = []
    for at in range(n_x):
        pieces.append(jnp.where(c == 0, column_abs[at], near_abs[at]))
        pieces.append(jnp.where(c == 0, near_abs[at], column_abs[at]))
    return jnp.concatenate(pieces, axis=0)


def rows_to_columns(own):
    n_tp = lax.axis_size("tp")
    n_x = n_tp // CORES
    tp = lax.axis_index("tp")
    x, c = tp // CORES, tp % CORES
    rows, cols = own.shape
    width = cols // n_tp
    result = jnp.zeros((n_tp * rows, width), own.dtype)
    for dx in range(n_x):
        for dc in range(CORES):
            to = (x + dx) % n_x * CORES + (c + dc) % CORES
            came = (x - dx) % n_x * CORES + (c - dc) % CORES
            block = lax.dynamic_slice_in_dim(own, to * width, width, 1)
            if dx or dc:
                block = move_tp(block, dx, dc)
            result = lax.dynamic_update_slice_in_dim(result, block, came * rows, 0)
    return result


def causal_taps(pre, taps):
    count = pre.shape[0] // SEQ
    blocks = pre.reshape(count, SEQ, pre.shape[1])
    padded = jnp.pad(blocks, ((0, 0), (2, 0), (0, 0)))
    result = padded[:, 0:SEQ] * taps[0] + padded[:, 1 : SEQ + 1] * taps[1] + padded[:, 2:] * taps[2]
    return result.reshape(pre.shape)


def mm(left, right):
    return jnp.dot(left, right, preferred_element_type=jnp.float32)


def split_norm(values, gain, width):
    sums = jnp.stack([jnp.sum(values, axis=1), jnp.sum(values * values, axis=1)])
    n_x = lax.axis_size("tp") // CORES
    total = sums
    for dx in range(n_x):
        for dc in range(CORES):
            if dx or dc:
                total = total + move_tp(sums, dx, dc)
    mean = total[0][:, None] / width
    spread = total[1][:, None] / width - mean * mean
    return (values - mean) * lax.rsqrt(spread + norm_eps) * gain


def per_device(
    tokens,
    w_gate_side,
    w_value_side,
    spatial_gain,
    w_spatial,
    spatial_bias,
    w_mixer_out,
    first_gain,
    w_ff_gate,
    w_ff_up,
    conv_gate_taps,
    conv_up_taps,
    w_ff_down,
    second_gain,
):
    rows, d = tokens.shape
    n_fs, n_tp = lax.axis_size("fs"), lax.axis_size("tp")
    n_y = n_fs // Z
    z = lax.axis_index("fs") // n_y
    tp = lax.axis_index("tp")
    shift = z * (d // Z)
    own_rows = rows // n_tp
    side = w_gate_side.shape[1]
    depth = w_gate_side.shape[0]

    near = y_blocks(jnp.concatenate([w_gate_side, w_value_side], axis=1))
    near_mix = y_blocks(w_mixer_out)
    sides = z_ring(jnp.concatenate(near, axis=0))
    mixes = z_ring(jnp.concatenate(near_mix, axis=1))
    gate_z = z_ring(w_ff_gate)
    gate_w = jnp.concatenate([b for s in gate_z for b in y_blocks(s)], axis=0)
    up_z = z_ring(w_ff_up)
    up_w = jnp.concatenate([b for s in up_z for b in y_blocks(s)], axis=0)
    down_z = z_ring(w_ff_down)
    down_w = [jnp.concatenate(y_blocks(s), axis=1) for s in down_z]

    tokens_rel = jnp.roll(tokens, -shift, axis=1)
    pre = mm(tokens_rel, jnp.concatenate(sides, axis=0))
    gate_act = jax.nn.gelu(pre[:, :side])
    value_norm = split_norm(
        jax.nn.gelu(pre[:, side:]), spatial_gain, side * n_tp
    ).astype(jnp.bfloat16)
    groups_dev = w_spatial.shape[0]
    blocks = value_norm.reshape(rows // SPAN, SPAN, groups_dev, GROUP_DIM)
    lower = jnp.tril(jnp.ones((SPAN, SPAN), jnp.bool_))
    causal_w = jnp.where(lower[None], w_spatial, jnp.zeros_like(w_spatial))
    mixed = jnp.einsum("gts,nsgc->ntgc", causal_w, blocks, preferred_element_type=jnp.float32)
    mixed = mixed + spatial_bias.T[None, :, :, None]
    spatial_out = (gate_act * mixed.reshape(rows, side)).astype(jnp.bfloat16)
    mixer_sum = scatter_rows(mm(spatial_out, jnp.concatenate(mixes, axis=1)))
    own_tokens = lax.dynamic_slice_in_dim(tokens_rel, tp * own_rows, own_rows, 0)
    first_own = row_norm(
        residual_scale * own_tokens.astype(jnp.float32) + mixer_sum, jnp.roll(first_gain, -shift)
    ).astype(jnp.bfloat16)
    first_whole = gather_rows(first_own)

    ff_gate = causal_taps(mm(first_whole, gate_w), conv_gate_taps)
    ff_up = causal_taps(mm(first_whole, up_w), conv_up_taps)
    ff_hidden = (jax.nn.silu(ff_gate) * ff_up).astype(jnp.bfloat16)
    ff_sum = jnp.concatenate([scatter_rows(mm(ff_hidden, piece)) for piece in down_w], axis=1)
    out_rel = row_norm(
        residual_scale * first_own.astype(jnp.float32) + ff_sum, jnp.roll(second_gain, -shift)
    ).astype(jnp.bfloat16)
    return rows_to_columns(jnp.roll(out_rel, shift, axis=1))


LANES = 128
KINDS = 10
SG, SV, MO, FG, FU, FD = 0, 1, 2, 3, 6, 9
CHUNKS = 3
PIECES = 4
MESH = pl.DeviceIdType.MESH
VMEM_BYTES = 67043328


def to_rows(column, rows):
    n = column.shape[0]
    return jnp.transpose(jnp.broadcast_to(column, (n, LANES)))[:rows]


def to_columns(row):
    return jnp.transpose(jnp.broadcast_to(row, (LANES, LANES)))


def stat_rows(first, second):
    a, b = to_rows(first, 8), to_rows(second, 8)
    at = lax.broadcasted_iota(jnp.int32, a.shape, 0)
    return jnp.where(at == 0, a, jnp.where(at == 1, b, 0.0))


def dotf(a, b):
    return jnp.dot(a, b, preferred_element_type=jnp.float32)


def layer_kernel(
    tokens,
    wgs,
    wvs,
    sgain,
    wsp,
    sbias,
    wmix,
    gain1,
    wgate,
    wup,
    taps_g,
    taps_u,
    wdown,
    gain2,
    out,
    tok,
    swg,
    swv,
    mo,
    wg,
    wu,
    wd,
    ga,
    va,
    so_own,
    so,
    yb,
    fn,
    h,
    s1,
    r1,
    s2,
    r2,
    s3,
    r3,
    keep,
    biasf,
    st,
    rst,
    rs_w,
    ss_z,
    ss_y,
    ss_mx,
    rs_mx,
    ss_mc,
    rs_mc,
    lsem,
    ss_st,
    rs_st,
    ss_so,
    rs_so,
    ss_t,
    rs_t,
    ss_c,
    rs_c,
    ss_x,
    rs_x,
    ss_e,
    rs_e,
):
    f, t = lax.axis_index("fs"), lax.axis_index("tp")
    z, y = f // 2, f % 2
    x, c = t // CORES, t % CORES
    zi = z % 2
    rows, d = tok.shape
    side = swg.shape[1]
    part = d // (2 * Z)
    hid = wgate.shape[1]
    window = wd.shape[1]
    cw = window // CHUNKS
    shift = hid - window
    half, quarter = rows // 2, rows // 4
    width2 = d // 4
    piece = 2 * rows // PIECES

    def far(k):
        if k == 1:
            return z + 1 - 2 * (z % 2)
        return (z + 2) % Z if k == 2 else Z - 1 - z

    def middle(at):
        return ((at + 1) // 2) % 2

    def offset(at):
        return pl.multiple_of(middle(at) * shift, LANES)

    me = (f, t)
    y_peer = (2 * z + 1 - y, t)
    x_peer = (f, (1 - x) * CORES + c)
    c_peer = (f, x * CORES + 1 - c)
    xc_peer = (f, (1 - x) * CORES + 1 - c)

    def z_peer(at):
        return (2 * at + y, t)

    tp_peers = (c_peer, x_peer, xc_peer)
    barrier = pltpu.get_barrier_semaphore()
    greeted = (y_peer,) + tp_peers + tuple(z_peer(far(k)) for k in (1, 2, 3))
    for peer in greeted:
        pl.semaphore_signal(barrier, inc=1, device_id=peer, device_id_type=MESH)
    pl.semaphore_wait(barrier, len(greeted))

    def remote(src, dst, ss, rs, to):
        return pltpu.make_async_remote_copy(
            src_ref=src, dst_ref=dst, send_sem=ss, recv_sem=rs, device_id=to, device_id_type=MESH
        )

    def source(kind, off):
        if kind == SG:
            return wgs
        if kind == SV:
            return wvs
        if kind == MO:
            return wmix
        if kind == FD:
            return wdown.at[pl.ds(off, window), :]
        ref = wgate if kind < FU else wup
        at = pl.multiple_of(off + ((kind - FG) % CHUNKS) * cw, LANES)
        return ref.at[:, pl.ds(at, cw)]

    def slot(kind, fsrc):
        at = pl.ds(pl.multiple_of(fsrc * part, part), part)
        if kind == SG:
            return swg.at[at, :]
        if kind == SV:
            return swv.at[at, :]
        if kind == MO:
            return mo.at[fsrc, pl.ds(pl.multiple_of(t * side, side), side), :]
        if kind == FD:
            return wd.at[fsrc]
        return (wg if kind < FU else wu).at[(kind - FG) % CHUNKS, at, :]

    drain = []

    def send(make, when=None):
        def go():
            make().start()

        def end():
            make().wait_send()

        if when is None:
            go()
            drain.append(end)
        else:
            pl.when(when)(go)
            drain.append(lambda: pl.when(when)(end))

    def arrive(kind, fsrc):
        ref = slot(kind, fsrc)
        remote(ref, ref, ss_y.at[kind, 0], rs_w.at[kind, fsrc], me).wait_recv()

    def own_local(kind):
        return pltpu.make_async_copy(source(kind, offset(z)), slot(kind, f), lsem.at[1 + kind])

    def own_y(kind):
        send(lambda: remote(source(kind, offset(z)), slot(kind, f), ss_y.at[kind, z], rs_w.at[kind, f], y_peer))

    def own_z(kind, k):
        to = far(k)
        send(lambda: remote(source(kind, offset(to)), slot(kind, f), ss_z.at[kind, k], rs_w.at[kind, f], z_peer(to)))

    def pass_y(kind, zs):
        fs = 2 * zs + y
        return lambda: remote(slot(kind, fs), slot(kind, fs), ss_y.at[kind, zs], rs_w.at[kind, fs], y_peer)

    def line_own(kind):
        send(lambda: remote(source(kind, 0), slot(kind, f), ss_z.at[kind, Z], rs_w.at[kind, f], z_peer(z + 1)), z < Z - 1)
        send(lambda: remote(source(kind, 0), slot(kind, f), ss_z.at[kind, z], rs_w.at[kind, f], z_peer(z - 1)), z > 0)

    def line_step(kinds, dist, also=None):
        for sign in (-1, 1):
            zs = z + sign * dist
            ok = (zs >= 0) & (zs < Z)
            on = ok & (z < Z - 1) if sign < 0 else ok & (z > 0)
            to = z - sign
            fs = 2 * zs + y
            for kind in kinds:

                def came(kind=kind, fs=fs):
                    arrive(kind, fs)

                pl.when(ok)(came)
                send(
                    lambda kind=kind, fs=fs, zs=zs, to=to: remote(
                        slot(kind, fs), slot(kind, fs), ss_z.at[kind, zs], rs_w.at[kind, fs], z_peer(to)
                    ),
                    on,
                )
                send(pass_y(kind, zs), ok)
                if also is not None:
                    also(fs, ok)

    def mix_x(fs, when=None):
        send(lambda: remote(slot(MO, fs), slot(MO, fs), ss_mx.at[fs], rs_mx.at[fs], x_peer), when)

    def relay_ff(kinds):
        for k in (1, 2, 3):
            for kind in kinds:
                arrive(kind, 2 * far(k) + y)
                send(pass_y(kind, far(k)))

    def settle(kinds):
        for kind in kinds:
            own_local(kind).wait()
            for zs in range(Z):
                arrive(kind, 2 * zs + 1 - y)

    load_tokens = pltpu.make_async_copy(tokens, tok, lsem.at[0])
    load_tokens.start()
    for kind in range(KINDS):
        own_local(kind).start()
    for kind in (SG, SV):
        line_own(kind)
    for kind in (SG, SV, MO):
        own_y(kind)
    line_own(MO)
    send(lambda: remote(wmix, slot(MO, f), ss_mx.at[f], rs_mx.at[f], x_peer))
    for chunk in (0, 1):
        for kind in (FG + chunk, FU + chunk):
            for k in (3, 2, 1):
                own_z(kind, k)
    for kind in (FG, FU):
        own_y(kind)
    for dist in (1, 2, 3):
        line_step((SG, SV), dist)

    lane2 = lax.broadcasted_iota(jnp.int32, (SPAN, side), 1) // GROUP_DIM
    groups = wsp.shape[0]
    bias_all = jnp.zeros((SPAN, side), jnp.float32)
    for g in range(groups):
        column = to_columns(sbias[g : g + 1, :])
        bias_all = jnp.where(lane2 == g, jnp.concatenate([column] * (side // LANES), axis=1), bias_all)
    biasf[...] = bias_all

    load_tokens.wait()
    settle((SG, SV))

    tile = 256

    @pl.loop(0, rows // tile)
    def _(i):
        at = pl.ds(pl.multiple_of(i * tile, tile), tile)
        a = tok[at, :]
        ga[at, :] = jax.nn.gelu(dotf(a, swg[...]))
        v = jax.nn.gelu(dotf(a, swv[...]))
        va[at, :] = v
        st[0, :, at] = stat_rows(jnp.sum(v, axis=1, keepdims=True), jnp.sum(v * v, axis=1, keepdims=True))

    def stats_out(n):
        for i, peer in enumerate(tp_peers):
            send(lambda i=i, peer=peer: remote(st.at[n], rst.at[n, i], ss_st.at[n, i], rs_st.at[n, i], peer))

    def stats_in(n):
        for i in range(3):
            remote(st.at[n], rst.at[n, i], ss_st.at[n, i], rs_st.at[n, i], me).wait_recv()

    def moments(n, at, width):
        total = st[n, :, at] + rst[n, 0, :, at] + rst[n, 1, :, at] + rst[n, 2, :, at]
        mean = total[0:1] / width
        spread = total[1:2] / width - mean * mean
        return to_columns(mean), to_columns(lax.rsqrt(spread + norm_eps))

    stats_out(0)
    for dist in (1, 2, 3):
        line_step((MO,), dist, mix_x)
    stats_in(0)

    @pl.loop(0, rows // SPAN)
    def _(n):
        at = pl.ds(pl.multiple_of(n * SPAN, SPAN), SPAN)
        mean, scale = moments(0, at, side * 2 * CORES)
        mean = jnp.concatenate([mean] * (side // LANES), axis=1)
        scale = jnp.concatenate([scale] * (side // LANES), axis=1)
        vn = ((va[at, :] - mean) * scale * sgain[...]).astype(jnp.bfloat16)
        low = lax.broadcasted_iota(jnp.int32, (SPAN, SPAN), 0) >= lax.broadcasted_iota(jnp.int32, (SPAN, SPAN), 1)
        group = lax.broadcasted_iota(jnp.int32, (SPAN, side), 1) // GROUP_DIM
        mixed = jnp.zeros((SPAN, side), jnp.float32)
        for g in range(groups):
            w = jnp.where(low, wsp[g].astype(jnp.float32), 0.0).astype(jnp.bfloat16)
            mixed = jnp.where(group == g, dotf(w, vn), mixed)
        so_own[at, :] = (ga[at, :] * (mixed + biasf[...])).astype(jnp.bfloat16)

    for i, peer in enumerate(tp_peers):
        to_c = 1 - c if i != 1 else c
        send(
            lambda i=i, peer=peer, to_c=to_c: remote(
                so_own.at[pl.ds(pl.multiple_of(to_c * half, half), half), :], so.at[t], ss_so.at[i], rs_so.at[i], peer
            )
        )
    mine = pl.multiple_of(c * half, half)
    so[t] = so_own[pl.ds(mine, half), :]

    own_local(MO).wait()
    for zs in range(Z):
        fs = 2 * zs + 1 - y
        arrive(MO, fs)
        mix_x(fs)
    for chunk in (1, 2):
        own_y(FG + chunk)
        own_y(FU + chunk)

    def mix_rows(at):
        return mo.at[:, pl.ds(pl.multiple_of(at * side, side), side), :]

    send(lambda: remote(mix_rows(t), mix_rows(t), ss_mc.at[0], rs_mc.at[0], c_peer))
    t_x = (1 - x) * CORES + c
    for fs in range(2 * Z):
        ref = mo.at[fs, pl.ds(pl.multiple_of(t_x * side, side), side), :]
        remote(ref, ref, ss_mx.at[fs], rs_mx.at[fs], me).wait_recv()
    send(lambda: remote(mix_rows(t_x), mix_rows(t_x), ss_mc.at[1], rs_mc.at[1], c_peer))
    for i, peer in enumerate(tp_peers):
        ref = so.at[peer[1]]
        remote(ref, ref, ss_so.at[i], rs_so.at[i], me).wait_recv()
    for i, at in enumerate((x * CORES + 1 - c, (1 - x) * CORES + 1 - c)):
        ref = mix_rows(at)
        remote(ref, ref, ss_mc.at[i], rs_mc.at[i], me).wait_recv()

    @pl.loop(0, 2 * Z)
    def _(fs):
        cols = pl.ds(pl.multiple_of(fs * part, part), part)
        acc = residual_scale * tok[pl.ds(mine, half), cols].astype(jnp.float32)
        for i in range(2 * CORES):
            acc += dotf(so[i], mo[fs, i * side : (i + 1) * side, :])
        yb[:, cols] = acc

    own0 = zi * rows
    strip = 32

    @pl.loop(0, half // strip)
    def _(i):
        at = pl.multiple_of(i * strip, strip)
        v = yb[pl.ds(at, strip), :]
        mean = jnp.sum(v, axis=1, keepdims=True) / d
        spread = jnp.sum(v * v, axis=1, keepdims=True) / d - mean * mean
        fn[pl.ds(pl.multiple_of(own0 + mine + at, strip), strip), :] = (
            (v - mean) * lax.rsqrt(spread + norm_eps) * gain1[...]
        ).astype(jnp.bfloat16)

    def token_rows(zz, cc, xx, p):
        n = quarter // 2
        at = zz * rows + cc * half + xx * quarter + p * n
        return fn.at[pl.ds(pl.multiple_of(at, n), n), :]

    def token_send(ref, i, peer):
        send(lambda: remote(ref(), ref(), ss_t.at[i], rs_t.at[i], peer))

    def token_wait(ref, i):
        remote(ref, ref, ss_t.at[i], rs_t.at[i], me).wait_recv()

    z_pair = z_peer(far(1))
    for p in (0, 1):
        token_send(lambda p=p: token_rows(zi, c, x, p), 1 + p, z_pair)

    def own_half(cc):
        return fn.at[pl.ds(pl.multiple_of(own0 + cc * half, half), half), :]

    token_send(lambda: own_half(c), 0, c_peer)
    for kind in (FG + 2, FU + 2, FD):
        for k in (3, 2, 1):
            own_z(kind, k)
    own_y(FD)

    def ff(j, base, tiles):
        n = 512

        @pl.loop(0, tiles)
        def _(i):
            at = pl.ds(pl.multiple_of(base + i * n, n), n)
            a = fn[at, :]
            row = lax.broadcasted_iota(jnp.int32, (n, cw), 0) % SEQ
            cols = pl.ds(pl.multiple_of(offset(z) + j * cw, LANES), cw)

            def conv(w, taps):
                p = dotf(a, w[j])
                one = jnp.where(row >= 1, pltpu.roll(p, 1, 0), 0.0)
                two = jnp.where(row >= 2, pltpu.roll(p, 2, 0), 0.0)
                return taps[0:1, cols] * two + taps[1:2, cols] * one + taps[2:3, cols] * p

            gate = conv(wg, taps_g)
            res = jax.nn.silu(gate) * conv(wu, taps_u)
            lane = lax.broadcasted_iota(jnp.int32, (n, cw), 1) + j * cw
            mine_too = lane < shift + middle(z) * (window - shift)
            h[j, at, :] = jnp.where(mine_too, res, 0.0).astype(jnp.bfloat16)

    other0 = (1 - zi) * rows
    relay_ff((FG, FU))
    token_wait(own_half(1 - c), 0)
    settle((FG, FU))
    ff(0, own0, rows // 512)
    for p in (0, 1):
        token_wait(token_rows(1 - zi, c, x, p), 1 + p)
        token_send(lambda p=p: token_rows(1 - zi, c, x, p), 3 + p, x_peer)
        token_send(lambda p=p: token_rows(1 - zi, c, x, p), 5 + p, c_peer)
    relay_ff((FG + 1, FU + 1))
    settle((FG + 1, FU + 1))
    ff(1, own0, rows // 512)
    for p in (0, 1):
        token_wait(token_rows(1 - zi, c, 1 - x, p), 3 + p)
        token_send(lambda p=p: token_rows(1 - zi, c, 1 - x, p), 7 + p, c_peer)
    relay_ff((FG + 2, FU + 2))
    for p in (0, 1):
        token_wait(token_rows(1 - zi, 1 - c, x, p), 5 + p)
        token_wait(token_rows(1 - zi, 1 - c, 1 - x, p), 7 + p)

    @pl.loop(0, 2)
    def _(j):
        ff(j, other0, rows // 512)

    settle((FG + 2, FU + 2))
    ff(2, 0, 2 * rows // 512)

    relay_ff((FD,))
    settle((FD,))

    def rr(q):
        return pl.ds(pl.multiple_of((other0 + q * piece) % (2 * rows), piece), piece)

    def product(q, zf, yy):
        w = wd.at[2 * zf + yy]
        acc = dotf(h[0, rr(q), :], w[0:cw, :])
        for j in range(1, CHUNKS):
            acc += dotf(h[j, rr(q), :], w[j * cw : (j + 1) * cw, :])
        return acc

    def core_copy(b, q):
        return remote(s1.at[b, q], r1.at[b, q], ss_c.at[b, q], rs_c.at[b, q], c_peer)

    def x_copy(q):
        return remote(s2.at[q], r2.at[q], ss_x.at[q], rs_x.at[q], x_peer)

    def z_copy(q):
        return remote(s3.at[q], r3.at[q], ss_e.at[q], rs_e.at[q], z_pair)

    @pl.loop(0, 2)
    def _(b):
        xo = x * b + (1 - x) * (1 - b)

        @pl.loop(0, PIECES)
        def _(q):
            for yy in (0, 1):
                s1[b, q, :, yy * part : (yy + 1) * part] = product(q, 2 * xo + 1 - c, yy).astype(jnp.bfloat16)
            core_copy(b, q).start()

        @pl.loop(0, PIECES)
        def _(q):
            own = [product(q, 2 * xo + c, yy) for yy in (0, 1)]
            core_copy(b, q).wait_recv()
            for yy in (0, 1):
                cols = slice(yy * part, (yy + 1) * part)
                keep[q, :, cols] = own[yy] + r1[b, q, :, cols].astype(jnp.float32)

            @pl.when(b == 0)
            def _():
                s2[q] = keep[q].astype(jnp.bfloat16)
                x_copy(q).start()

    @pl.loop(0, PIECES // 2)
    def _(q):
        x_copy(q).wait_recv()
        s3[q] = (keep[q] + r2[q].astype(jnp.float32)).astype(jnp.bfloat16)
        z_copy(q).start()

    out_cols = pl.ds(pl.multiple_of(t * width2, width2), width2)

    @pl.loop(0, PIECES // 2)
    def _(q):
        x_copy(q + PIECES // 2).wait_recv()
        z_copy(q).wait_recv()
        v = keep[q + PIECES // 2] + r2[q + PIECES // 2].astype(jnp.float32) + r3[q].astype(jnp.float32)
        v += residual_scale * fn[rr(q + PIECES // 2), out_cols].astype(jnp.float32)
        keep[q + PIECES // 2] = v
        st[1, :, pl.ds(pl.multiple_of(q * piece, piece), piece)] = stat_rows(
            jnp.sum(v, axis=1, keepdims=True), jnp.sum(v * v, axis=1, keepdims=True)
        )

    stats_out(1)
    stats_in(1)

    @pl.loop(0, rows // LANES)
    def _(n):
        at = pl.ds(pl.multiple_of(n * LANES, LANES), LANES)
        mean, scale = moments(1, at, d)
        mean = jnp.concatenate([mean] * (width2 // LANES), axis=1)
        scale = jnp.concatenate([scale] * (width2 // LANES), axis=1)
        per = piece // LANES
        v = keep[PIECES // 2 + n // per, pl.ds(pl.multiple_of((n % per) * LANES, LANES), LANES), :]
        out[at, :] = ((v - mean) * scale * gain2[:, out_cols]).astype(jnp.bfloat16)

    @pl.loop(0, PIECES)
    def _(q):
        core_copy(0, q).wait_send()
        core_copy(1, q).wait_send()
        x_copy(q).wait_send()

    @pl.loop(0, PIECES // 2)
    def _(q):
        z_copy(q).wait_send()

    for end in drain:
        end()


def per_device_small(
    tokens,
    w_gate_side,
    w_value_side,
    spatial_gain,
    w_spatial,
    spatial_bias,
    w_mixer_out,
    first_gain,
    w_ff_gate,
    w_ff_up,
    conv_gate_taps,
    conv_up_taps,
    w_ff_down,
    second_gain,
):
    rows, d = tokens.shape
    side = w_gate_side.shape[1]
    n_fs = lax.axis_size("fs")
    part = d // n_fs
    hid = w_ff_gate.shape[1]
    window = -(-hid // (2 * LANES)) * LANES
    cw = window // CHUNKS
    piece = 2 * rows // PIECES
    width2 = d // lax.axis_size("tp")
    bf, f32 = jnp.bfloat16, jnp.float32
    vmem, dma = pltpu.VMEM, pltpu.SemaphoreType.DMA
    anywhere = pl.BlockSpec(memory_space=pl.ANY)
    local = pl.BlockSpec(memory_space=pltpu.VMEM)
    return pl.pallas_call(
        layer_kernel,
        out_shape=jax.ShapeDtypeStruct((rows, width2), bf),
        in_specs=[
            anywhere,
            anywhere,
            anywhere,
            local,
            local,
            local,
            anywhere,
            local,
            anywhere,
            anywhere,
            local,
            local,
            anywhere,
            local,
        ],
        out_specs=local,
        scratch_shapes=[
            vmem((rows, d), bf),
            vmem((d, side), bf),
            vmem((d, side), bf),
            vmem((n_fs, side * 2 * CORES, part), bf),
            vmem((CHUNKS, d, cw), bf),
            vmem((CHUNKS, d, cw), bf),
            vmem((n_fs, window, part), bf),
            vmem((rows, side), f32),
            vmem((rows, side), f32),
            vmem((rows, side), bf),
            vmem((2 * CORES, rows // 2, side), bf),
            vmem((rows // 2, d), f32),
            vmem((2 * rows, d), bf),
            vmem((CHUNKS, 2 * rows, cw), bf),
            vmem((2, PIECES, piece, width2), bf),
            vmem((2, PIECES, piece, width2), bf),
            vmem((PIECES, piece, width2), bf),
            vmem((PIECES, piece, width2), bf),
            vmem((PIECES // 2, piece, width2), bf),
            vmem((PIECES // 2, piece, width2), bf),
            vmem((PIECES, piece, width2), f32),
            vmem((SPAN, side), f32),
            vmem((2, 8, rows), f32),
            vmem((2, 3, 8, rows), f32),
            dma((KINDS, n_fs)),
            dma((KINDS, Z + 1)),
            dma((KINDS, Z)),
            dma((n_fs,)),
            dma((n_fs,)),
            dma((2,)),
            dma((2,)),
            dma((1 + KINDS,)),
            dma((2, 3)),
            dma((2, 3)),
            dma((3,)),
            dma((3,)),
            dma((9,)),
            dma((9,)),
            dma((2, PIECES)),
            dma((2, PIECES)),
            dma((PIECES,)),
            dma((PIECES,)),
            dma((PIECES // 2,)),
            dma((PIECES // 2,)),
        ],
        compiler_params=pltpu.CompilerParams(
            collective_id=0, has_side_effects=True, vmem_limit_bytes=VMEM_BYTES
        ),
        name="layer",
    )(
        tokens,
        w_gate_side,
        w_value_side,
        spatial_gain.reshape(1, -1),
        w_spatial,
        spatial_bias,
        w_mixer_out,
        first_gain.reshape(1, -1),
        w_ff_gate,
        w_ff_up,
        conv_gate_taps,
        conv_up_taps,
        w_ff_down,
        second_gain.reshape(1, -1),
    )


def solution(mesh):
    small = mesh.shape["fs"] == 2 * Z and mesh.shape["tp"] == 2 * CORES
    body = per_device_small if small else per_device
    return jax.shard_map(
        body,
        mesh=mesh,
        in_specs=(
            P("fs", None),
            P("fs", "tp"),
            P("fs", "tp"),
            P("tp"),
            P("tp", None, None),
            P("tp", None),
            P("tp", "fs"),
            P(),
            P("fs", "tp"),
            P("fs", "tp"),
            P(None, "tp"),
            P(None, "tp"),
            P("tp", "fs"),
            P(),
        ),
        out_specs=P("fs", "tp"),
        check_vma=False,
    )
```

```python
import jax
import jax.numpy as jnp
from jax import lax
from jax.experimental import pallas as pl
from jax.experimental.pallas import tpu as pltpu
from jax.sharding import PartitionSpec as P

GROUP_DIM = 64
SPAN = 128
SEQ = 256
Z = 4
CORES = 2

residual_scale = 2.0**0.25
norm_eps = 1e-05


def fs_pairs(n_fs, dz, dy):
    n_y = n_fs // Z
    pairs = []
    for index in range(n_fs):
        z, y = index // n_y, index % n_y
        pairs.append((index, (z + dz) % Z * n_y + (y + dy) % n_y))
    return pairs


def tp_pairs(n_tp, dx, dc):
    n_x = n_tp // CORES
    pairs = []
    for index in range(n_tp):
        x, c = index // CORES, index % CORES
        pairs.append((index, (x + dx) % n_x * CORES + (c + dc) % CORES))
    return pairs


def move_fs(value, dz, dy):
    return lax.ppermute(value, "fs", fs_pairs(lax.axis_size("fs"), dz, dy))


def move_tp(value, dx, dc):
    return lax.ppermute(value, "tp", tp_pairs(lax.axis_size("tp"), dx, dc))


def y_blocks(own):
    n_y = lax.axis_size("fs") // Z
    y = lax.axis_index("fs") % n_y
    pieces = [own]
    for step in range(1, n_y):
        pieces.append(move_fs(pieces[-1], 0, 1))
    return [lax.select_n((y - at) % n_y, *pieces) if n_y > 2 else lax.select_n((y - at) % n_y == 1, *pieces) for at in range(n_y)]


def z_ring(own):
    right = move_fs(own, 1, 0)
    left = move_fs(own, -1, 0)
    far = move_fs(right, 1, 0)
    return [own, left, far, right]


def row_norm(values, gain):
    width = values.shape[1]
    mean = jnp.sum(values, axis=1, keepdims=True) / width
    spread = jnp.sum(values * values, axis=1, keepdims=True) / width - mean * mean
    return (values - mean) * lax.rsqrt(spread + norm_eps) * gain


def scatter_rows(part):
    n_tp = lax.axis_size("tp")
    n_x = n_tp // CORES
    tp = lax.axis_index("tp")
    x, c = tp // CORES, tp % CORES
    rows, cols = part.shape
    blocks = part.astype(jnp.bfloat16).reshape(n_x, CORES, rows // n_tp, cols)
    mine = lax.dynamic_index_in_dim(blocks, c, 1, keepdims=False)
    other = lax.dynamic_index_in_dim(blocks, 1 - c, 1, keepdims=False)
    pair = mine.astype(jnp.float32) + move_tp(other, 0, 1).astype(jnp.float32)
    total = lax.dynamic_index_in_dim(pair, x, 0, keepdims=False)
    for dx in range(1, n_x):
        away = lax.dynamic_index_in_dim(pair, (x + dx) % n_x, 0, keepdims=False)
        total = total + move_tp(away.astype(jnp.bfloat16), dx, 0).astype(jnp.float32)
    return total


def gather_rows(own):
    n_tp = lax.axis_size("tp")
    n_x = n_tp // CORES
    tp = lax.axis_index("tp")
    x, c = tp // CORES, tp % CORES
    column = [own]
    for dx in range(1, n_x):
        column.append(move_tp(own, dx, 0))
    column_abs = [
        lax.select_n((x - at) % n_x == 1, *column) if n_x == 2 else lax.select_n((x - at) % n_x, *column)
        for at in range(n_x)
    ]
    near = [move_tp(value, 0, 1) for value in column]
    near_abs = [
        lax.select_n((x - at) % n_x == 1, *near) if n_x == 2 else lax.select_n((x - at) % n_x, *near)
        for at in range(n_x)
    ]
    pieces = []
    for at in range(n_x):
        pieces.append(jnp.where(c == 0, column_abs[at], near_abs[at]))
        pieces.append(jnp.where(c == 0, near_abs[at], column_abs[at]))
    return jnp.concatenate(pieces, axis=0)


def rows_to_columns(own):
    n_tp = lax.axis_size("tp")
    n_x = n_tp // CORES
    tp = lax.axis_index("tp")
    x, c = tp // CORES, tp % CORES
    rows, cols = own.shape
    width = cols // n_tp
    result = jnp.zeros((n_tp * rows, width), own.dtype)
    for dx in range(n_x):
        for dc in range(CORES):
            to = (x + dx) % n_x * CORES + (c + dc) % CORES
            came = (x - dx) % n_x * CORES + (c - dc) % CORES
            block = lax.dynamic_slice_in_dim(own, to * width, width, 1)
            if dx or dc:
                block = move_tp(block, dx, dc)
            result = lax.dynamic_update_slice_in_dim(result, block, came * rows, 0)
    return result


def causal_taps(pre, taps):
    count = pre.shape[0] // SEQ
    blocks = pre.reshape(count, SEQ, pre.shape[1])
    padded = jnp.pad(blocks, ((0, 0), (2, 0), (0, 0)))
    result = padded[:, 0:SEQ] * taps[0] + padded[:, 1 : SEQ + 1] * taps[1] + padded[:, 2:] * taps[2]
    return result.reshape(pre.shape)


def mm(left, right):
    return jnp.dot(left, right, preferred_element_type=jnp.float32)


def split_norm(values, gain, width):
    sums = jnp.stack([jnp.sum(values, axis=1), jnp.sum(values * values, axis=1)])
    n_x = lax.axis_size("tp") // CORES
    total = sums
    for dx in range(n_x):
        for dc in range(CORES):
            if dx or dc:
                total = total + move_tp(sums, dx, dc)
    mean = total[0][:, None] / width
    spread = total[1][:, None] / width - mean * mean
    return (values - mean) * lax.rsqrt(spread + norm_eps) * gain


def per_device(
    tokens,
    w_gate_side,
    w_value_side,
    spatial_gain,
    w_spatial,
    spatial_bias,
    w_mixer_out,
    first_gain,
    w_ff_gate,
    w_ff_up,
    conv_gate_taps,
    conv_up_taps,
    w_ff_down,
    second_gain,
):
    rows, d = tokens.shape
    n_fs, n_tp = lax.axis_size("fs"), lax.axis_size("tp")
    n_y = n_fs // Z
    z = lax.axis_index("fs") // n_y
    tp = lax.axis_index("tp")
    shift = z * (d // Z)
    own_rows = rows // n_tp
    side = w_gate_side.shape[1]
    depth = w_gate_side.shape[0]

    near = y_blocks(jnp.concatenate([w_gate_side, w_value_side], axis=1))
    near_mix = y_blocks(w_mixer_out)
    sides = z_ring(jnp.concatenate(near, axis=0))
    mixes = z_ring(jnp.concatenate(near_mix, axis=1))
    gate_z = z_ring(w_ff_gate)
    gate_w = jnp.concatenate([b for s in gate_z for b in y_blocks(s)], axis=0)
    up_z = z_ring(w_ff_up)
    up_w = jnp.concatenate([b for s in up_z for b in y_blocks(s)], axis=0)
    down_z = z_ring(w_ff_down)
    down_w = [jnp.concatenate(y_blocks(s), axis=1) for s in down_z]

    tokens_rel = jnp.roll(tokens, -shift, axis=1)
    pre = mm(tokens_rel, jnp.concatenate(sides, axis=0))
    gate_act = jax.nn.gelu(pre[:, :side])
    value_norm = split_norm(
        jax.nn.gelu(pre[:, side:]), spatial_gain, side * n_tp
    ).astype(jnp.bfloat16)
    groups_dev = w_spatial.shape[0]
    blocks = value_norm.reshape(rows // SPAN, SPAN, groups_dev, GROUP_DIM)
    lower = jnp.tril(jnp.ones((SPAN, SPAN), jnp.bool_))
    causal_w = jnp.where(lower[None], w_spatial, jnp.zeros_like(w_spatial))
    mixed = jnp.einsum("gts,nsgc->ntgc", causal_w, blocks, preferred_element_type=jnp.float32)
    mixed = mixed + spatial_bias.T[None, :, :, None]
    spatial_out = (gate_act * mixed.reshape(rows, side)).astype(jnp.bfloat16)
    mixer_sum = scatter_rows(mm(spatial_out, jnp.concatenate(mixes, axis=1)))
    own_tokens = lax.dynamic_slice_in_dim(tokens_rel, tp * own_rows, own_rows, 0)
    first_own = row_norm(
        residual_scale * own_tokens.astype(jnp.float32) + mixer_sum, jnp.roll(first_gain, -shift)
    ).astype(jnp.bfloat16)
    first_whole = gather_rows(first_own)

    ff_gate = causal_taps(mm(first_whole, gate_w), conv_gate_taps)
    ff_up = causal_taps(mm(first_whole, up_w), conv_up_taps)
    ff_hidden = (jax.nn.silu(ff_gate) * ff_up).astype(jnp.bfloat16)
    ff_sum = jnp.concatenate([scatter_rows(mm(ff_hidden, piece)) for piece in down_w], axis=1)
    out_rel = row_norm(
        residual_scale * first_own.astype(jnp.float32) + ff_sum, jnp.roll(second_gain, -shift)
    ).astype(jnp.bfloat16)
    return rows_to_columns(jnp.roll(out_rel, shift, axis=1))


LANES = 128
KINDS = 10
SG, SV, MO, FG, FU, FD = 0, 1, 2, 3, 6, 9
CHUNKS = 3
PIECES = 4
TOKEN_PIECES = 4
MESH = pl.DeviceIdType.MESH
VMEM_BYTES = 67043328


def to_rows(column, rows):
    n = column.shape[0]
    return jnp.transpose(jnp.broadcast_to(column, (n, LANES)))[:rows]


def to_columns(row):
    return jnp.transpose(jnp.broadcast_to(row, (LANES, LANES)))


def stat_rows(first, second):
    a, b = to_rows(first, 8), to_rows(second, 8)
    at = lax.broadcasted_iota(jnp.int32, a.shape, 0)
    return jnp.where(at == 0, a, jnp.where(at == 1, b, 0.0))


def dotf(a, b):
    return jnp.dot(a, b, preferred_element_type=jnp.float32)


def layer_kernel(
    tokens,
    wgs,
    wvs,
    sgain,
    wsp,
    sbias,
    wmix,
    gain1,
    wgate,
    wup,
    taps_g,
    taps_u,
    wdown,
    gain2,
    out,
    tok,
    swg,
    swv,
    mo,
    wg,
    wu,
    wd,
    ga,
    va,
    so_own,
    so,
    yb,
    fn,
    h,
    s1,
    r1,
    s2,
    r2,
    s3,
    r3,
    keep,
    keep_x,
    biasf,
    st,
    rst,
    rs_w,
    ss_z,
    ss_y,
    ss_mx,
    rs_mx,
    ss_mc,
    rs_mc,
    lsem,
    ss_st,
    rs_st,
    ss_so,
    rs_so,
    ss_t,
    rs_t,
    ss_c,
    rs_c,
    ss_x,
    rs_x,
    ss_e,
    rs_e,
):
    f, t = lax.axis_index("fs"), lax.axis_index("tp")
    z, y = f // 2, f % 2
    x, c = t // CORES, t % CORES
    zi = z % 2
    rows, d = tok.shape
    side = swg.shape[1]
    part = d // (2 * Z)
    hid = wgate.shape[1]
    window = wd.shape[1]
    cw = window // CHUNKS
    shift = hid - window
    half, quarter = rows // 2, rows // 4
    width2 = d // 4
    piece = 2 * rows // PIECES

    def far(k):
        if k == 1:
            return z + 1 - 2 * (z % 2)
        return (z + 2) % Z if k == 2 else Z - 1 - z

    def middle(at):
        return ((at + 1) // 2) % 2

    def offset(at):
        return pl.multiple_of(middle(at) * shift, LANES)

    me = (f, t)
    y_peer = (2 * z + 1 - y, t)
    x_peer = (f, (1 - x) * CORES + c)
    c_peer = (f, x * CORES + 1 - c)
    xc_peer = (f, (1 - x) * CORES + 1 - c)

    def z_peer(at):
        return (2 * at + y, t)

    tp_peers = (c_peer, x_peer, xc_peer)
    barrier = pltpu.get_barrier_semaphore()
    greeted = (y_peer,) + tp_peers + tuple(z_peer(far(k)) for k in (1, 2, 3))
    for peer in greeted:
        pl.semaphore_signal(barrier, inc=1, device_id=peer, device_id_type=MESH)
    pl.semaphore_wait(barrier, len(greeted))

    def remote(src, dst, ss, rs, to):
        return pltpu.make_async_remote_copy(
            src_ref=src, dst_ref=dst, send_sem=ss, recv_sem=rs, device_id=to, device_id_type=MESH
        )

    outer = middle(z) == 0
    inner = middle(z) == 1

    def cut(kind):
        if kind == FD:
            return shift
        return min(cw, shift - ((kind - FG) % CHUNKS) * cw) if kind >= FG else None

    def varies(kind):
        return kind >= FG and cut(kind) != (window if kind == FD else cw)

    def source(kind, off, narrow=False):
        if kind == SG:
            return wgs
        if kind == SV:
            return wvs
        if kind == MO:
            return wmix
        if kind == FD:
            return wdown.at[pl.ds(off, cut(kind) if narrow else window), :]
        ref = wgate if kind < FU else wup
        at = pl.multiple_of(off + ((kind - FG) % CHUNKS) * cw, LANES)
        return ref.at[:, pl.ds(at, cut(kind) if narrow else cw)]

    def slot(kind, fsrc, narrow=False):
        at = pl.ds(pl.multiple_of(fsrc * part, part), part)
        if kind == SG:
            return swg.at[at, :]
        if kind == SV:
            return swv.at[at, :]
        if kind == MO:
            return mo.at[fsrc, pl.ds(pl.multiple_of(t * side, side), side), :]
        if kind == FD:
            return wd.at[fsrc, pl.ds(0, cut(kind) if narrow else window), :]
        return (wg if kind < FU else wu).at[(kind - FG) % CHUNKS, at, pl.ds(0, cut(kind) if narrow else cw)]

    drain = []

    def guard(when, role):
        return role if when is None else when & role

    def run(when, act):
        if when is None:
            act()
        else:
            pl.when(when)(act)

    def send(make, when=None):
        run(when, lambda: make().start())
        drain.append(lambda: run(when, lambda: make().wait_send()))

    def by_role(kind, act, when=None):
        if varies(kind):
            act(False, guard(when, inner))
            act(True, guard(when, outer))
        else:
            act(False, when)

    def arrive(kind, fsrc, when=None):
        def act(narrow, on):
            ref = slot(kind, fsrc, narrow)
            run(on, lambda: remote(ref, ref, ss_y.at[kind, 0], rs_w.at[kind, fsrc], me).wait_recv())

        by_role(kind, act, when)

    def own_local(kind, narrow):
        return pltpu.make_async_copy(source(kind, offset(z), narrow), slot(kind, f, narrow), lsem.at[1 + kind])

    def own_start(kind):
        by_role(kind, lambda narrow, on: run(on, lambda: own_local(kind, narrow).start()))

    def own_wait(kind, when=None):
        by_role(kind, lambda narrow, on: run(on, lambda: own_local(kind, narrow).wait()), when)

    def own_y(kind):
        by_role(
            kind,
            lambda narrow, on: send(
                lambda: remote(
                    source(kind, offset(z), narrow), slot(kind, f, narrow), ss_y.at[kind, z], rs_w.at[kind, f], y_peer
                ),
                on,
            ),
        )

    def own_z(kind, k, when, narrow):
        to = far(k)
        narrow = narrow and varies(kind)
        send(
            lambda: remote(
                source(kind, offset(to), narrow), slot(kind, f, narrow), ss_z.at[kind, k], rs_w.at[kind, f], z_peer(to)
            ),
            when,
        )

    def pass_y(kind, zs, when=None):
        fs = 2 * zs + y

        def act(narrow, on):
            send(
                lambda: remote(
                    slot(kind, fs, narrow), slot(kind, fs, narrow), ss_y.at[kind, zs], rs_w.at[kind, fs], y_peer
                ),
                on,
            )

        by_role(kind, act, when)

    def line_own(kind):
        send(lambda: remote(source(kind, 0), slot(kind, f), ss_z.at[kind, Z], rs_w.at[kind, f], z_peer(z + 1)), z < Z - 1)
        send(lambda: remote(source(kind, 0), slot(kind, f), ss_z.at[kind, z], rs_w.at[kind, f], z_peer(z - 1)), z > 0)

    def line_step(kinds, dist, also=None):
        for sign in (-1, 1):
            zs = z + sign * dist
            ok = (zs >= 0) & (zs < Z)
            on = ok & (z < Z - 1) if sign < 0 else ok & (z > 0)
            to = z - sign
            fs = 2 * zs + y
            for kind in kinds:

                def came(kind=kind, fs=fs):
                    arrive(kind, fs)

                pl.when(ok)(came)
                send(
                    lambda kind=kind, fs=fs, zs=zs, to=to: remote(
                        slot(kind, fs), slot(kind, fs), ss_z.at[kind, zs], rs_w.at[kind, fs], z_peer(to)
                    ),
                    on,
                )
                pass_y(kind, zs, ok)
                if kind == MO and also is not None:
                    also(fs, ok)

    def mix_x(fs, when=None):
        send(lambda: remote(slot(MO, fs), slot(MO, fs), ss_mx.at[fs], rs_mx.at[fs], x_peer), when)

    def relay_ff(kinds):
        for k in (1, 2, 3):
            for kind in kinds:
                arrive(kind, 2 * far(k) + y)
                pass_y(kind, far(k))

    def settle(kinds):
        for kind in kinds:
            own_wait(kind)
            for zs in range(Z):
                arrive(kind, 2 * zs + 1 - y)

    load_tokens = pltpu.make_async_copy(tokens, tok, lsem.at[0])
    load_tokens.start()
    for kind in range(KINDS):
        own_start(kind)
    for kind in (SG, SV, MO):
        line_own(kind)
        own_y(kind)
    send(lambda: remote(wmix, slot(MO, f), ss_mx.at[f], rs_mx.at[f], x_peer))

    @pl.when(outer)
    def _():
        wd[:, shift:, :] = jnp.zeros((2 * Z, window - shift, part), wd.dtype)
        for ref in (wg, wu):
            ref[CHUNKS - 1, :, cut(FU - 1) :] = jnp.zeros((d, window - shift), ref.dtype)

    def to_middle(kinds):
        for kind in kinds:
            own_z(kind, 3, inner, False)
            own_z(kind, 2, outer, False)
            own_z(kind, 1, outer, False)

    def to_ends(kinds, hops=(3, 2, 1)):
        for kind in kinds:
            for k in hops:
                own_z(kind, k, outer if k == 3 else inner, True)


    def mix_y_to_x(dist):
        for sign in (-1, 1) if dist else (1,):
            zs = z + sign * dist
            ok = (zs >= 0) & (zs < Z)
            fs = 2 * zs + 1 - y
            pl.when(ok)(lambda fs=fs: arrive(MO, fs))
            mix_x(fs, ok)

    line_step((SG, SV, MO), 1, mix_x)
    to_middle((FG, FU))
    mix_y_to_x(0)
    line_step((SG, SV, MO), 2, mix_x)
    to_ends((FG, FU), (1,))
    mix_y_to_x(1)
    line_step((SG, SV, MO), 3, mix_x)
    for chunk in range(CHUNKS):
        own_y(FG + chunk)
        own_y(FU + chunk)

    lane2 = lax.broadcasted_iota(jnp.int32, (SPAN, side), 1) // GROUP_DIM
    groups = wsp.shape[0]
    bias_all = jnp.zeros((SPAN, side), jnp.float32)
    for g in range(groups):
        column = to_columns(sbias[g : g + 1, :])
        bias_all = jnp.where(lane2 == g, jnp.concatenate([column] * (side // LANES), axis=1), bias_all)
    biasf[...] = bias_all

    load_tokens.wait()
    settle((SG, SV))
    to_ends((FG, FU), (3, 2))
    for chunk in range(1, CHUNKS):
        to_middle((FG + chunk, FU + chunk))
        to_ends((FG + chunk, FU + chunk))

    tile = 256

    @pl.loop(0, rows // tile)
    def _(i):
        at = pl.ds(pl.multiple_of(i * tile, tile), tile)
        a = tok[at, :]
        ga[at, :] = jax.nn.gelu(dotf(a, swg[...]))
        v = jax.nn.gelu(dotf(a, swv[...]))
        va[at, :] = v
        st[0, :, at] = stat_rows(jnp.sum(v, axis=1, keepdims=True), jnp.sum(v * v, axis=1, keepdims=True))

    def stats_out(n):
        for i, peer in enumerate(tp_peers):
            send(lambda i=i, peer=peer: remote(st.at[n], rst.at[n, i], ss_st.at[n, i], rs_st.at[n, i], peer))

    def stats_in(n):
        for i in range(3):
            remote(st.at[n], rst.at[n, i], ss_st.at[n, i], rs_st.at[n, i], me).wait_recv()

    def moments(n, at, width):
        total = st[n, :, at] + rst[n, 0, :, at] + rst[n, 1, :, at] + rst[n, 2, :, at]
        mean = total[0:1] / width
        spread = total[1:2] / width - mean * mean
        return to_columns(mean), to_columns(lax.rsqrt(spread + norm_eps))

    stats_out(0)
    own_wait(MO)
    mix_y_to_x(2)
    mix_y_to_x(3)
    stats_in(0)

    @pl.loop(0, rows // SPAN)
    def _(n):
        at = pl.ds(pl.multiple_of(n * SPAN, SPAN), SPAN)
        mean, scale = moments(0, at, side * 2 * CORES)
        mean = jnp.concatenate([mean] * (side // LANES), axis=1)
        scale = jnp.concatenate([scale] * (side // LANES), axis=1)
        vn = ((va[at, :] - mean) * scale * sgain[...]).astype(jnp.bfloat16)
        low = lax.broadcasted_iota(jnp.int32, (SPAN, SPAN), 0) >= lax.broadcasted_iota(jnp.int32, (SPAN, SPAN), 1)
        group = lax.broadcasted_iota(jnp.int32, (SPAN, side), 1) // GROUP_DIM
        mixed = jnp.zeros((SPAN, side), jnp.float32)
        for g in range(groups):
            w = jnp.where(low, wsp[g].astype(jnp.float32), 0.0).astype(jnp.bfloat16)
            mixed = jnp.where(group == g, dotf(w, vn), mixed)
        so_own[at, :] = (ga[at, :] * (mixed + biasf[...])).astype(jnp.bfloat16)

    for i, peer in enumerate(tp_peers):
        to_c = 1 - c if i != 1 else c
        send(
            lambda i=i, peer=peer, to_c=to_c: remote(
                so_own.at[pl.ds(pl.multiple_of(to_c * half, half), half), :], so.at[t], ss_so.at[i], rs_so.at[i], peer
            )
        )
    mine = pl.multiple_of(c * half, half)
    so[t] = so_own[pl.ds(mine, half), :]

    def mix_rows(at):
        return mo.at[:, pl.ds(pl.multiple_of(at * side, side), side), :]

    send(lambda: remote(mix_rows(t), mix_rows(t), ss_mc.at[0], rs_mc.at[0], c_peer))
    t_x = (1 - x) * CORES + c
    for fs in range(2 * Z):
        ref = mo.at[fs, pl.ds(pl.multiple_of(t_x * side, side), side), :]
        remote(ref, ref, ss_mx.at[fs], rs_mx.at[fs], me).wait_recv()
    send(lambda: remote(mix_rows(t_x), mix_rows(t_x), ss_mc.at[1], rs_mc.at[1], c_peer))
    relay_ff((FG, FU))
    for i, peer in enumerate(tp_peers):
        ref = so.at[peer[1]]
        remote(ref, ref, ss_so.at[i], rs_so.at[i], me).wait_recv()
    for i, at in enumerate((x * CORES + 1 - c, (1 - x) * CORES + 1 - c)):
        ref = mix_rows(at)
        remote(ref, ref, ss_mc.at[i], rs_mc.at[i], me).wait_recv()

    @pl.loop(0, 2 * Z)
    def _(fs):
        cols = pl.ds(pl.multiple_of(fs * part, part), part)
        acc = residual_scale * tok[pl.ds(mine, half), cols].astype(jnp.float32)
        for i in range(2 * CORES):
            acc += dotf(so[i], mo[fs, i * side : (i + 1) * side, :])
        yb[:, cols] = acc

    own0 = zi * rows
    strip = 32

    @pl.loop(0, half // strip)
    def _(i):
        at = pl.multiple_of(i * strip, strip)
        v = yb[pl.ds(at, strip), :]
        mean = jnp.sum(v, axis=1, keepdims=True) / d
        spread = jnp.sum(v * v, axis=1, keepdims=True) / d - mean * mean
        fn[pl.ds(pl.multiple_of(own0 + mine + at, strip), strip), :] = (
            (v - mean) * lax.rsqrt(spread + norm_eps) * gain1[...]
        ).astype(jnp.bfloat16)

    tp_n = TOKEN_PIECES

    def token_rows(zz, cc, xx, p):
        n = quarter // tp_n
        at = zz * rows + cc * half + xx * quarter + p * n
        return fn.at[pl.ds(pl.multiple_of(at, n), n), :]

    def token_send(ref, i, peer):
        send(lambda: remote(ref(), ref(), ss_t.at[i], rs_t.at[i], peer))

    def token_wait(ref, i):
        remote(ref, ref, ss_t.at[i], rs_t.at[i], me).wait_recv()

    z_pair = z_peer(far(1))
    for p in range(tp_n):
        token_send(lambda p=p: token_rows(zi, c, x, p), 1 + p, z_pair)

    def own_half(cc):
        return fn.at[pl.ds(pl.multiple_of(own0 + cc * half, half), half), :]

    token_send(lambda: own_half(c), 0, c_peer)
    to_middle((FD,))
    relay_ff((FG + 1, FU + 1))

    def ff(j, base, tiles):
        n = 512

        @pl.loop(0, tiles)
        def _(i):
            at = pl.ds(pl.multiple_of(base + i * n, n), n)
            a = fn[at, :]
            row = lax.broadcasted_iota(jnp.int32, (n, cw), 0) % SEQ
            cols = pl.ds(pl.multiple_of(offset(z) + j * cw, LANES), cw)

            def conv(w, taps):
                p = dotf(a, w[j])
                one = jnp.where(row >= 1, pltpu.roll(p, 1, 0), 0.0)
                two = jnp.where(row >= 2, pltpu.roll(p, 2, 0), 0.0)
                return taps[0:1, cols] * two + taps[1:2, cols] * one + taps[2:3, cols] * p

            gate = conv(wg, taps_g)
            res = jax.nn.silu(gate) * conv(wu, taps_u)
            lane = lax.broadcasted_iota(jnp.int32, (n, cw), 1) + j * cw
            mine_too = lane < shift + middle(z) * (window - shift)
            h[j, at, :] = jnp.where(mine_too, res, 0.0).astype(jnp.bfloat16)

    other0 = (1 - zi) * rows

    def down_pass(hops):
        for k in hops:
            arrive(FD, 2 * far(k) + y)
            pass_y(FD, far(k))

    def down_ready(stage):
        if stage == 0:
            own_wait(FD)
        for zs in [2 * (z // 2 if stage == 0 else 1 - z // 2) + i for i in (0, 1)]:
            arrive(FD, 2 * zs + 1 - y)

    token_wait(own_half(1 - c), 0)
    settle((FG, FU))
    ff(0, own0, rows // 512)
    relay_ff((FG + 2, FU + 2))
    own_y(FD)
    for p in range(tp_n):
        token_wait(token_rows(1 - zi, c, x, p), 1 + p)
        token_send(lambda p=p: token_rows(1 - zi, c, x, p), 1 + tp_n + p, x_peer)
        token_send(lambda p=p: token_rows(1 - zi, c, x, p), 1 + 2 * tp_n + p, c_peer)
    to_ends((FD,))
    settle((FG + 1, FU + 1))
    ff(1, own0, rows // 512)
    settle((FG + 2, FU + 2))
    ff(2, own0, rows // 512)
    down_pass((1,))
    for p in range(tp_n):
        token_wait(token_rows(1 - zi, c, 1 - x, p), 1 + tp_n + p)
        token_send(lambda p=p: token_rows(1 - zi, c, 1 - x, p), 1 + 3 * tp_n + p, c_peer)
    for p in range(tp_n):
        token_wait(token_rows(1 - zi, 1 - c, x, p), 1 + 2 * tp_n + p)
        token_wait(token_rows(1 - zi, 1 - c, 1 - x, p), 1 + 3 * tp_n + p)

    down_pass((2, 3))
    @pl.loop(0, CHUNKS)
    def _(j):
        ff(j, other0, rows // 512)

    def rr(q):
        return pl.ds(pl.multiple_of((other0 + q * piece) % (2 * rows), piece), piece)

    def product(q, zf, yy):
        w = wd.at[2 * zf + yy]
        acc = dotf(h[0, rr(q), :], w[0:cw, :])
        for j in range(1, CHUNKS):
            acc += dotf(h[j, rr(q), :], w[j * cw : (j + 1) * cw, :])
        return acc

    def core_copy(b, q):
        return remote(s1.at[b, q], r1.at[b, q], ss_c.at[b, q], rs_c.at[b, q], c_peer)

    def x_copy(q):
        return remote(s2.at[q], r2.at[q], ss_x.at[q], rs_x.at[q], x_peer)

    def z_copy(q):
        return remote(s3.at[q], r3.at[q], ss_e.at[q], rs_e.at[q], z_pair)

    half_pieces = PIECES // 2

    def reduce_core(stage):
        xo = z // 2 if stage == 0 else 1 - z // 2
        b = jnp.where(xo == x, 1, 0)

        @pl.loop(0, PIECES)
        def _(q):
            for yy in (0, 1):
                s1[b, q, :, yy * part : (yy + 1) * part] = product(q, 2 * xo + 1 - c, yy).astype(jnp.bfloat16)
            core_copy(b, q).start()

        @pl.loop(0, PIECES)
        def _(q):
            own = [product(q, 2 * xo + c, yy) for yy in (0, 1)]
            core_copy(b, q).wait_recv()
            first, second = [
                own[yy] + r1[b, q, :, yy * part : (yy + 1) * part].astype(jnp.float32) for yy in (0, 1)
            ]

            @pl.when(b == 1)
            def _():
                keep[q, :, :part] = first
                keep[q, :, part:] = second

            @pl.when(b == 0)
            def _():
                s2[q] = first.astype(jnp.bfloat16)
                x_copy(q).start()

            @pl.when(q < half_pieces)
            def _():
                s3[half_pieces * b + q] = second.astype(jnp.bfloat16)
                z_copy(half_pieces * b + q).start()

            @pl.when((b == 0) & (q >= half_pieces))
            def _():
                keep_x[q - half_pieces] = second

    down_ready(0)
    reduce_core(0)
    down_ready(1)
    reduce_core(1)

    @pl.loop(0, half_pieces)
    def _(q):
        z_copy(q).wait_recv()
        s2[PIECES + q] = (keep_x[q] + r3[q].astype(jnp.float32)).astype(jnp.bfloat16)
        x_copy(PIECES + q).start()

    @pl.loop(0, half_pieces)
    def _(q):
        x_copy(q).wait_recv()
        s3[2 * half_pieces + q] = (keep[q, :, :part] + r2[q].astype(jnp.float32)).astype(jnp.bfloat16)
        z_copy(2 * half_pieces + q).start()

    out_cols = pl.ds(pl.multiple_of(t * width2, width2), width2)

    @pl.loop(0, PIECES // 2)
    def _(q):
        own_piece = q + half_pieces
        z_copy(half_pieces + q).wait_recv()
        x_copy(own_piece).wait_recv()
        z_copy(2 * half_pieces + q).wait_recv()
        x_copy(PIECES + q).wait_recv()
        first = r2[own_piece].astype(jnp.float32) + r3[2 * half_pieces + q].astype(jnp.float32)
        second = r2[PIECES + q].astype(jnp.float32) + r3[half_pieces + q].astype(jnp.float32)
        v = keep[own_piece] + jnp.concatenate([first, second], axis=1)
        v += residual_scale * fn[rr(q + PIECES // 2), out_cols].astype(jnp.float32)
        keep[q + PIECES // 2] = v
        st[1, :, pl.ds(pl.multiple_of(q * piece, piece), piece)] = stat_rows(
            jnp.sum(v, axis=1, keepdims=True), jnp.sum(v * v, axis=1, keepdims=True)
        )

    stats_out(1)
    stats_in(1)

    @pl.loop(0, rows // LANES)
    def _(n):
        at = pl.ds(pl.multiple_of(n * LANES, LANES), LANES)
        mean, scale = moments(1, at, d)
        mean = jnp.concatenate([mean] * (width2 // LANES), axis=1)
        scale = jnp.concatenate([scale] * (width2 // LANES), axis=1)
        per = piece // LANES
        v = keep[PIECES // 2 + n // per, pl.ds(pl.multiple_of((n % per) * LANES, LANES), LANES), :]
        out[at, :] = ((v - mean) * scale * gain2[:, out_cols]).astype(jnp.bfloat16)

    @pl.loop(0, PIECES)
    def _(q):
        core_copy(0, q).wait_send()
        core_copy(1, q).wait_send()

    @pl.loop(0, 3 * half_pieces)
    def _(q):
        x_copy(q).wait_send()
        z_copy(q).wait_send()

    for end in drain:
        end()


def per_device_small(
    tokens,
    w_gate_side,
    w_value_side,
    spatial_gain,
    w_spatial,
    spatial_bias,
    w_mixer_out,
    first_gain,
    w_ff_gate,
    w_ff_up,
    conv_gate_taps,
    conv_up_taps,
    w_ff_down,
    second_gain,
):
    rows, d = tokens.shape
    side = w_gate_side.shape[1]
    n_fs = lax.axis_size("fs")
    part = d // n_fs
    hid = w_ff_gate.shape[1]
    window = -(-hid // (2 * LANES)) * LANES
    cw = window // CHUNKS
    piece = 2 * rows // PIECES
    width2 = d // lax.axis_size("tp")
    bf, f32 = jnp.bfloat16, jnp.float32
    vmem, dma = pltpu.VMEM, pltpu.SemaphoreType.DMA
    anywhere = pl.BlockSpec(memory_space=pl.ANY)
    local = pl.BlockSpec(memory_space=pltpu.VMEM)
    return pl.pallas_call(
        layer_kernel,
        out_shape=jax.ShapeDtypeStruct((rows, width2), bf),
        in_specs=[
            anywhere,
            anywhere,
            anywhere,
            local,
            local,
            local,
            anywhere,
            local,
            anywhere,
            anywhere,
            local,
            local,
            anywhere,
            local,
        ],
        out_specs=local,
        scratch_shapes=[
            vmem((rows, d), bf),
            vmem((d, side), bf),
            vmem((d, side), bf),
            vmem((n_fs, side * 2 * CORES, part), bf),
            vmem((CHUNKS, d, cw), bf),
            vmem((CHUNKS, d, cw), bf),
            vmem((n_fs, window, part), bf),
            vmem((rows, side), f32),
            vmem((rows, side), f32),
            vmem((rows, side), bf),
            vmem((2 * CORES, rows // 2, side), bf),
            vmem((rows // 2, d), f32),
            vmem((2 * rows, d), bf),
            vmem((CHUNKS, 2 * rows, cw), bf),
            vmem((2, PIECES, piece, width2), bf),
            vmem((2, PIECES, piece, width2), bf),
            vmem((3 * PIECES // 2, piece, part), bf),
            vmem((3 * PIECES // 2, piece, part), bf),
            vmem((3 * PIECES // 2, piece, part), bf),
            vmem((3 * PIECES // 2, piece, part), bf),
            vmem((PIECES, piece, width2), f32),
            vmem((PIECES // 2, piece, part), f32),
            vmem((SPAN, side), f32),
            vmem((2, 8, rows), f32),
            vmem((2, 3, 8, rows), f32),
            dma((KINDS, n_fs)),
            dma((KINDS, Z + 1)),
            dma((KINDS, Z)),
            dma((n_fs,)),
            dma((n_fs,)),
            dma((2,)),
            dma((2,)),
            dma((1 + KINDS,)),
            dma((2, 3)),
            dma((2, 3)),
            dma((3,)),
            dma((3,)),
            dma((1 + 4 * TOKEN_PIECES,)),
            dma((1 + 4 * TOKEN_PIECES,)),
            dma((2, PIECES)),
            dma((2, PIECES)),
            dma((3 * PIECES // 2,)),
            dma((3 * PIECES // 2,)),
            dma((3 * PIECES // 2,)),
            dma((3 * PIECES // 2,)),
        ],
        compiler_params=pltpu.CompilerParams(
            collective_id=0, has_side_effects=True, vmem_limit_bytes=VMEM_BYTES
        ),
        name="layer",
    )(
        tokens,
        w_gate_side,
        w_value_side,
        spatial_gain.reshape(1, -1),
        w_spatial,
        spatial_bias,
        w_mixer_out,
        first_gain.reshape(1, -1),
        w_ff_gate,
        w_ff_up,
        conv_gate_taps,
        conv_up_taps,
        w_ff_down,
        second_gain.reshape(1, -1),
    )


def solution(mesh):
    small = mesh.shape["fs"] == 2 * Z and mesh.shape["tp"] == 2 * CORES
    body = per_device_small if small else per_device
    return jax.shard_map(
        body,
        mesh=mesh,
        in_specs=(
            P("fs", None),
            P("fs", "tp"),
            P("fs", "tp"),
            P("tp"),
            P("tp", None, None),
            P("tp", None),
            P("tp", "fs"),
            P(),
            P("fs", "tp"),
            P("fs", "tp"),
            P(None, "tp"),
            P(None, "tp"),
            P("tp", "fs"),
            P(),
        ),
        out_specs=P("fs", "tp"),
        check_vma=False,
    )
```

```python
import jax
import jax.numpy as jnp
from jax import lax
from jax.experimental import pallas as pl
from jax.experimental.pallas import tpu as pltpu
from jax.sharding import PartitionSpec as P

GROUP_DIM = 64
SPAN = 128
SEQ = 256
Z = 4
CORES = 2

residual_scale = 2.0**0.25
norm_eps = 1e-05


def fs_pairs(n_fs, dz, dy):
    n_y = n_fs // Z
    pairs = []
    for index in range(n_fs):
        z, y = index // n_y, index % n_y
        pairs.append((index, (z + dz) % Z * n_y + (y + dy) % n_y))
    return pairs


def tp_pairs(n_tp, dx, dc):
    n_x = n_tp // CORES
    pairs = []
    for index in range(n_tp):
        x, c = index // CORES, index % CORES
        pairs.append((index, (x + dx) % n_x * CORES + (c + dc) % CORES))
    return pairs


def move_fs(value, dz, dy):
    return lax.ppermute(value, "fs", fs_pairs(lax.axis_size("fs"), dz, dy))


def move_tp(value, dx, dc):
    return lax.ppermute(value, "tp", tp_pairs(lax.axis_size("tp"), dx, dc))


def y_blocks(own):
    n_y = lax.axis_size("fs") // Z
    y = lax.axis_index("fs") % n_y
    pieces = [own]
    for step in range(1, n_y):
        pieces.append(move_fs(pieces[-1], 0, 1))
    return [lax.select_n((y - at) % n_y, *pieces) if n_y > 2 else lax.select_n((y - at) % n_y == 1, *pieces) for at in range(n_y)]


def z_ring(own):
    right = move_fs(own, 1, 0)
    left = move_fs(own, -1, 0)
    far = move_fs(right, 1, 0)
    return [own, left, far, right]


def row_norm(values, gain):
    width = values.shape[1]
    mean = jnp.sum(values, axis=1, keepdims=True) / width
    spread = jnp.sum(values * values, axis=1, keepdims=True) / width - mean * mean
    return (values - mean) * lax.rsqrt(spread + norm_eps) * gain


def scatter_rows(part):
    n_tp = lax.axis_size("tp")
    n_x = n_tp // CORES
    tp = lax.axis_index("tp")
    x, c = tp // CORES, tp % CORES
    rows, cols = part.shape
    blocks = part.astype(jnp.bfloat16).reshape(n_x, CORES, rows // n_tp, cols)
    mine = lax.dynamic_index_in_dim(blocks, c, 1, keepdims=False)
    other = lax.dynamic_index_in_dim(blocks, 1 - c, 1, keepdims=False)
    pair = mine.astype(jnp.float32) + move_tp(other, 0, 1).astype(jnp.float32)
    total = lax.dynamic_index_in_dim(pair, x, 0, keepdims=False)
    for dx in range(1, n_x):
        away = lax.dynamic_index_in_dim(pair, (x + dx) % n_x, 0, keepdims=False)
        total = total + move_tp(away.astype(jnp.bfloat16), dx, 0).astype(jnp.float32)
    return total


def gather_rows(own):
    n_tp = lax.axis_size("tp")
    n_x = n_tp // CORES
    tp = lax.axis_index("tp")
    x, c = tp // CORES, tp % CORES
    column = [own]
    for dx in range(1, n_x):
        column.append(move_tp(own, dx, 0))
    column_abs = [
        lax.select_n((x - at) % n_x == 1, *column) if n_x == 2 else lax.select_n((x - at) % n_x, *column)
        for at in range(n_x)
    ]
    near = [move_tp(value, 0, 1) for value in column]
    near_abs = [
        lax.select_n((x - at) % n_x == 1, *near) if n_x == 2 else lax.select_n((x - at) % n_x, *near)
        for at in range(n_x)
    ]
    pieces = []
    for at in range(n_x):
        pieces.append(jnp.where(c == 0, column_abs[at], near_abs[at]))
        pieces.append(jnp.where(c == 0, near_abs[at], column_abs[at]))
    return jnp.concatenate(pieces, axis=0)


def rows_to_columns(own):
    n_tp = lax.axis_size("tp")
    n_x = n_tp // CORES
    tp = lax.axis_index("tp")
    x, c = tp // CORES, tp % CORES
    rows, cols = own.shape
    width = cols // n_tp
    result = jnp.zeros((n_tp * rows, width), own.dtype)
    for dx in range(n_x):
        for dc in range(CORES):
            to = (x + dx) % n_x * CORES + (c + dc) % CORES
            came = (x - dx) % n_x * CORES + (c - dc) % CORES
            block = lax.dynamic_slice_in_dim(own, to * width, width, 1)
            if dx or dc:
                block = move_tp(block, dx, dc)
            result = lax.dynamic_update_slice_in_dim(result, block, came * rows, 0)
    return result


def causal_taps(pre, taps):
    count = pre.shape[0] // SEQ
    blocks = pre.reshape(count, SEQ, pre.shape[1])
    padded = jnp.pad(blocks, ((0, 0), (2, 0), (0, 0)))
    result = padded[:, 0:SEQ] * taps[0] + padded[:, 1 : SEQ + 1] * taps[1] + padded[:, 2:] * taps[2]
    return result.reshape(pre.shape)


def mm(left, right):
    return jnp.dot(left, right, preferred_element_type=jnp.float32)


def split_norm(values, gain, width):
    sums = jnp.stack([jnp.sum(values, axis=1), jnp.sum(values * values, axis=1)])
    n_x = lax.axis_size("tp") // CORES
    total = sums
    for dx in range(n_x):
        for dc in range(CORES):
            if dx or dc:
                total = total + move_tp(sums, dx, dc)
    mean = total[0][:, None] / width
    spread = total[1][:, None] / width - mean * mean
    return (values - mean) * lax.rsqrt(spread + norm_eps) * gain


def per_device(
    tokens,
    w_gate_side,
    w_value_side,
    spatial_gain,
    w_spatial,
    spatial_bias,
    w_mixer_out,
    first_gain,
    w_ff_gate,
    w_ff_up,
    conv_gate_taps,
    conv_up_taps,
    w_ff_down,
    second_gain,
):
    rows, d = tokens.shape
    n_fs, n_tp = lax.axis_size("fs"), lax.axis_size("tp")
    n_y = n_fs // Z
    z = lax.axis_index("fs") // n_y
    tp = lax.axis_index("tp")
    shift = z * (d // Z)
    own_rows = rows // n_tp
    side = w_gate_side.shape[1]
    depth = w_gate_side.shape[0]

    near = y_blocks(jnp.concatenate([w_gate_side, w_value_side], axis=1))
    near_mix = y_blocks(w_mixer_out)
    sides = z_ring(jnp.concatenate(near, axis=0))
    mixes = z_ring(jnp.concatenate(near_mix, axis=1))
    gate_z = z_ring(w_ff_gate)
    gate_w = jnp.concatenate([b for s in gate_z for b in y_blocks(s)], axis=0)
    up_z = z_ring(w_ff_up)
    up_w = jnp.concatenate([b for s in up_z for b in y_blocks(s)], axis=0)
    down_z = z_ring(w_ff_down)
    down_w = [jnp.concatenate(y_blocks(s), axis=1) for s in down_z]

    tokens_rel = jnp.roll(tokens, -shift, axis=1)
    pre = mm(tokens_rel, jnp.concatenate(sides, axis=0))
    gate_act = jax.nn.gelu(pre[:, :side])
    value_norm = split_norm(
        jax.nn.gelu(pre[:, side:]), spatial_gain, side * n_tp
    ).astype(jnp.bfloat16)
    groups_dev = w_spatial.shape[0]
    blocks = value_norm.reshape(rows // SPAN, SPAN, groups_dev, GROUP_DIM)
    lower = jnp.tril(jnp.ones((SPAN, SPAN), jnp.bool_))
    causal_w = jnp.where(lower[None], w_spatial, jnp.zeros_like(w_spatial))
    mixed = jnp.einsum("gts,nsgc->ntgc", causal_w, blocks, preferred_element_type=jnp.float32)
    mixed = mixed + spatial_bias.T[None, :, :, None]
    spatial_out = (gate_act * mixed.reshape(rows, side)).astype(jnp.bfloat16)
    mixer_sum = scatter_rows(mm(spatial_out, jnp.concatenate(mixes, axis=1)))
    own_tokens = lax.dynamic_slice_in_dim(tokens_rel, tp * own_rows, own_rows, 0)
    first_own = row_norm(
        residual_scale * own_tokens.astype(jnp.float32) + mixer_sum, jnp.roll(first_gain, -shift)
    ).astype(jnp.bfloat16)
    first_whole = gather_rows(first_own)

    ff_gate = causal_taps(mm(first_whole, gate_w), conv_gate_taps)
    ff_up = causal_taps(mm(first_whole, up_w), conv_up_taps)
    ff_hidden = (jax.nn.silu(ff_gate) * ff_up).astype(jnp.bfloat16)
    ff_sum = jnp.concatenate([scatter_rows(mm(ff_hidden, piece)) for piece in down_w], axis=1)
    out_rel = row_norm(
        residual_scale * first_own.astype(jnp.float32) + ff_sum, jnp.roll(second_gain, -shift)
    ).astype(jnp.bfloat16)
    return rows_to_columns(jnp.roll(out_rel, shift, axis=1))


LANES = 128
CHUNKS = 3
SG, SV, MO, FG, FU, FD = 0, 1, 2, 3, 3 + CHUNKS, 3 + 2 * CHUNKS
KINDS = 3 + 3 * CHUNKS
DOWN = tuple(range(FD, KINDS))
PIECES = 4
TOKEN_PIECES = 4
MESH = pl.DeviceIdType.MESH
VMEM_BYTES = 67043328


def to_rows(column, rows):
    n = column.shape[0]
    return jnp.transpose(jnp.broadcast_to(column, (n, LANES)))[:rows]


def to_columns(row):
    return jnp.transpose(jnp.broadcast_to(row, (LANES, LANES)))


def stat_rows(first, second):
    a, b = to_rows(first, 8), to_rows(second, 8)
    at = lax.broadcasted_iota(jnp.int32, a.shape, 0)
    return jnp.where(at == 0, a, jnp.where(at == 1, b, 0.0))


def dotf(a, b):
    return jnp.dot(a, b, preferred_element_type=jnp.float32)


def layer_kernel(
    tokens,
    wgs,
    wvs,
    sgain_in,
    wsp_in,
    sbias_in,
    wmix,
    gain1_in,
    wgate,
    wup,
    taps_g_in,
    taps_u_in,
    wdown,
    gain2_in,
    out,
    sgain,
    wsp,
    sbias,
    gain1,
    taps_g,
    taps_u,
    gain2,
    tok,
    swg,
    swv,
    mo,
    wg,
    wu,
    wd,
    ga,
    va,
    so_own,
    so,
    yb,
    fn,
    h,
    s1,
    r1,
    s2,
    r2,
    s3,
    r3,
    keep,
    keep_x,
    biasf,
    st,
    rst,
    rs_w,
    ss_z,
    ss_y,
    ss_mx,
    rs_mx,
    ss_mc,
    rs_mc,
    lsem,
    ss_st,
    rs_st,
    ss_so,
    rs_so,
    ss_t,
    rs_t,
    ss_c,
    rs_c,
    ss_x,
    rs_x,
    ss_e,
    rs_e,
):
    f, t = lax.axis_index("fs"), lax.axis_index("tp")
    z, y = f // 2, f % 2
    x, c = t // CORES, t % CORES
    zi = z % 2
    rows, d = tok.shape
    side = swg.shape[1]
    part = d // (2 * Z)
    hid = wgate.shape[1]
    window = wd.shape[1]
    cw = window // CHUNKS
    shift = hid - window
    half, quarter = rows // 2, rows // 4
    width2 = d // 4
    piece = 2 * rows // PIECES

    def far(k):
        if k == 1:
            return z + 1 - 2 * (z % 2)
        return (z + 2) % Z if k == 2 else Z - 1 - z

    def middle(at):
        return ((at + 1) // 2) % 2

    def offset(at):
        return pl.multiple_of(middle(at) * shift, LANES)

    me = (f, t)
    y_peer = (2 * z + 1 - y, t)
    x_peer = (f, (1 - x) * CORES + c)
    c_peer = (f, x * CORES + 1 - c)
    xc_peer = (f, (1 - x) * CORES + 1 - c)

    def z_peer(at):
        return (2 * at + y, t)

    tp_peers = (c_peer, x_peer, xc_peer)
    barrier = pltpu.get_barrier_semaphore()
    greeted = (y_peer,) + tp_peers + tuple(z_peer(far(k)) for k in (1, 2, 3))
    for peer in greeted:
        pl.semaphore_signal(barrier, inc=1, device_id=peer, device_id_type=MESH)
    pl.semaphore_wait(barrier, len(greeted))

    def remote(src, dst, ss, rs, to):
        return pltpu.make_async_remote_copy(
            src_ref=src, dst_ref=dst, send_sem=ss, recv_sem=rs, device_id=to, device_id_type=MESH
        )

    late = z // 2 == x
    early = z // 2 != x
    outer = middle(z) == 0
    inner = middle(z) == 1

    def cut(kind):
        return min(cw, shift - ((kind - FG) % CHUNKS) * cw)

    def varies(kind):
        return kind >= FG and cut(kind) != cw

    def source(kind, off, narrow=False):
        if kind == SG:
            return wgs
        if kind == SV:
            return wvs
        if kind == MO:
            return wmix
        at = pl.multiple_of(off + ((kind - FG) % CHUNKS) * cw, LANES)
        cols = pl.ds(at, cut(kind) if narrow else cw)
        if kind >= FD:
            return wdown.at[cols, :]
        return (wgate if kind < FU else wup).at[:, cols]

    def slot(kind, fsrc, narrow=False):
        at = pl.ds(pl.multiple_of(fsrc * part, part), part)
        if kind == SG:
            return swg.at[at, :]
        if kind == SV:
            return swv.at[at, :]
        if kind == MO:
            return mo.at[fsrc, pl.ds(pl.multiple_of(t * side, side), side), :]
        if kind >= FD:
            return wd.at[fsrc, pl.ds((kind - FD) * cw, cut(kind) if narrow else cw), :]
        return (wg if kind < FU else wu).at[(kind - FG) % CHUNKS, at, pl.ds(0, cut(kind) if narrow else cw)]

    drain = []

    def guard(when, role):
        return role if when is None else when & role

    def run(when, act):
        if when is None:
            act()
        else:
            pl.when(when)(act)

    def send(make, when=None):
        run(when, lambda: make().start())
        drain.append(lambda: run(when, lambda: make().wait_send()))

    def by_role(kind, act, when=None):
        if varies(kind):
            act(False, guard(when, inner))
            act(True, guard(when, outer))
        else:
            act(False, when)

    def arrive(kind, fsrc, when=None):
        def act(narrow, on):
            ref = slot(kind, fsrc, narrow)
            run(on, lambda: remote(ref, ref, ss_y.at[kind, 0], rs_w.at[kind, fsrc], me).wait_recv())

        by_role(kind, act, when)

    def own_local(kind, narrow):
        return pltpu.make_async_copy(source(kind, offset(z), narrow), slot(kind, f, narrow), lsem.at[1 + kind])

    def own_start(kind):
        by_role(kind, lambda narrow, on: run(on, lambda: own_local(kind, narrow).start()))

    def own_wait(kind, when=None):
        by_role(kind, lambda narrow, on: run(on, lambda: own_local(kind, narrow).wait()), when)

    def own_y(kind, when=None):
        by_role(
            kind,
            lambda narrow, on: send(
                lambda: remote(
                    source(kind, offset(z), narrow), slot(kind, f, narrow), ss_y.at[kind, z], rs_w.at[kind, f], y_peer
                ),
                on,
            ),
            when,
        )

    def own_z(kind, k, when, narrow):
        to = far(k)
        narrow = narrow and varies(kind)
        send(
            lambda: remote(
                source(kind, offset(to), narrow), slot(kind, f, narrow), ss_z.at[kind, k], rs_w.at[kind, f], z_peer(to)
            ),
            when,
        )

    def pass_y(kind, zs, when=None):
        fs = 2 * zs + y

        def act(narrow, on):
            send(
                lambda: remote(
                    slot(kind, fs, narrow), slot(kind, fs, narrow), ss_y.at[kind, zs], rs_w.at[kind, fs], y_peer
                ),
                on,
            )

        by_role(kind, act, when)

    def line_own(kind):
        send(lambda: remote(source(kind, 0), slot(kind, f), ss_z.at[kind, Z], rs_w.at[kind, f], z_peer(z + 1)), z < Z - 1)
        send(lambda: remote(source(kind, 0), slot(kind, f), ss_z.at[kind, z], rs_w.at[kind, f], z_peer(z - 1)), z > 0)

    def line_step(kinds, dist, also=None):
        for sign in (-1, 1):
            zs = z + sign * dist
            ok = (zs >= 0) & (zs < Z)
            on = ok & (z < Z - 1) if sign < 0 else ok & (z > 0)
            to = z - sign
            fs = 2 * zs + y
            for kind in kinds:

                def came(kind=kind, fs=fs):
                    arrive(kind, fs)

                pl.when(ok)(came)
                send(
                    lambda kind=kind, fs=fs, zs=zs, to=to: remote(
                        slot(kind, fs), slot(kind, fs), ss_z.at[kind, zs], rs_w.at[kind, fs], z_peer(to)
                    ),
                    on,
                )
                pass_y(kind, zs, ok)
                if kind == MO and also is not None:
                    also(fs, ok)

    def mix_x(fs, when=None):
        send(lambda: remote(slot(MO, fs), slot(MO, fs), ss_mx.at[fs], rs_mx.at[fs], x_peer), when)

    def relay_ff(kinds):
        for k in (1, 2, 3):
            for kind in kinds:
                arrive(kind, 2 * far(k) + y)
                pass_y(kind, far(k))

    def settle(kinds):
        for kind in kinds:
            own_wait(kind)
            for zs in range(Z):
                arrive(kind, 2 * zs + 1 - y)

    load_tokens = pltpu.make_async_copy(tokens, tok, lsem.at[0])
    load_tokens.start()
    small = [
        pltpu.make_async_copy(src, dst, lsem.at[1 + KINDS + i])
        for i, (src, dst) in enumerate(
            (
                (sgain_in, sgain),
                (wsp_in, wsp),
                (sbias_in, sbias),
                (gain1_in, gain1),
                (taps_g_in, taps_g),
                (taps_u_in, taps_u),
                (gain2_in, gain2),
            )
        )
    ]
    for kind in (SG, SV, MO):
        line_own(kind)
        own_y(kind)
    for kind in range(KINDS):
        own_start(kind)
    send(lambda: remote(wmix, slot(MO, f), ss_mx.at[f], rs_mx.at[f], x_peer))
    for copy in small:
        copy.start()

    def to_middle(kinds, when=None):
        for kind in kinds:
            own_z(kind, 3, guard(when, inner), False)
            own_z(kind, 2, guard(when, outer), False)
            own_z(kind, 1, guard(when, outer), False)

    def to_ends(kinds, hops=(3, 2, 1), when=None):
        for kind in kinds:
            for k in hops:
                own_z(kind, k, guard(when, outer if k == 3 else inner), True)

    def mix_y_to_x(dist):
        for sign in (-1, 1) if dist else (1,):
            zs = z + sign * dist
            ok = (zs >= 0) & (zs < Z)
            fs = 2 * zs + 1 - y
            pl.when(ok)(lambda fs=fs: arrive(MO, fs))
            mix_x(fs, ok)

    @pl.when(outer)
    def _():
        wd[:, shift:, :] = jnp.zeros((2 * Z, window - shift, part), wd.dtype)
        for ref in (wg, wu):
            ref[CHUNKS - 1, :, cut(FU - 1) :] = jnp.zeros((d, window - shift), ref.dtype)

    line_step((SG, SV, MO), 1, mix_x)
    mix_y_to_x(0)
    line_step((SG, SV, MO), 2, mix_x)
    to_middle((FG, FU))
    mix_y_to_x(1)
    line_step((SG, SV, MO), 3, mix_x)
    to_ends((FG, FU))
    to_middle((FG + 1, FU + 1))
    to_ends((FG + 1, FU + 1))
    to_middle((FG + 2, FU + 2))
    to_ends((FG + 2, FU + 2))
    for chunk in range(CHUNKS):
        own_y(FG + chunk)
        own_y(FU + chunk)

    for copy in small:
        copy.wait()

    lane2 = lax.broadcasted_iota(jnp.int32, (SPAN, side), 1) // GROUP_DIM
    groups = wsp.shape[0]
    bias_all = jnp.zeros((SPAN, side), jnp.float32)
    for g in range(groups):
        column = to_columns(sbias[g : g + 1, :])
        bias_all = jnp.where(lane2 == g, jnp.concatenate([column] * (side // LANES), axis=1), bias_all)
    biasf[...] = bias_all

    load_tokens.wait()
    settle((SG, SV))

    tile = 256

    @pl.loop(0, rows // tile)
    def _(i):
        at = pl.ds(pl.multiple_of(i * tile, tile), tile)
        a = tok[at, :]
        ga[at, :] = jax.nn.gelu(dotf(a, swg[...]))
        v = jax.nn.gelu(dotf(a, swv[...]))
        va[at, :] = v
        st[0, :, at] = stat_rows(jnp.sum(v, axis=1, keepdims=True), jnp.sum(v * v, axis=1, keepdims=True))

    def stats_out(n):
        for i, peer in enumerate(tp_peers):
            send(lambda i=i, peer=peer: remote(st.at[n], rst.at[n, i], ss_st.at[n, i], rs_st.at[n, i], peer))

    def stats_in(n):
        for i in range(3):
            remote(st.at[n], rst.at[n, i], ss_st.at[n, i], rs_st.at[n, i], me).wait_recv()

    def moments(n, at, width):
        total = st[n, :, at] + rst[n, 0, :, at] + rst[n, 1, :, at] + rst[n, 2, :, at]
        mean = total[0:1] / width
        spread = total[1:2] / width - mean * mean
        return to_columns(mean), to_columns(lax.rsqrt(spread + norm_eps))

    stats_out(0)
    own_wait(MO)
    mix_y_to_x(2)
    mix_y_to_x(3)
    stats_in(0)

    @pl.loop(0, rows // SPAN)
    def _(n):
        at = pl.ds(pl.multiple_of(n * SPAN, SPAN), SPAN)
        mean, scale = moments(0, at, side * 2 * CORES)
        mean = jnp.concatenate([mean] * (side // LANES), axis=1)
        scale = jnp.concatenate([scale] * (side // LANES), axis=1)
        vn = ((va[at, :] - mean) * scale * sgain[...]).astype(jnp.bfloat16)
        low = lax.broadcasted_iota(jnp.int32, (SPAN, SPAN), 0) >= lax.broadcasted_iota(jnp.int32, (SPAN, SPAN), 1)
        group = lax.broadcasted_iota(jnp.int32, (SPAN, side), 1) // GROUP_DIM
        mixed = jnp.zeros((SPAN, side), jnp.float32)
        for g in range(groups):
            w = jnp.where(low, wsp[g].astype(jnp.float32), 0.0).astype(jnp.bfloat16)
            mixed = jnp.where(group == g, dotf(w, vn), mixed)
        so_own[at, :] = (ga[at, :] * (mixed + biasf[...])).astype(jnp.bfloat16)

    for i, peer in enumerate(tp_peers):
        to_c = 1 - c if i != 1 else c
        send(
            lambda i=i, peer=peer, to_c=to_c: remote(
                so_own.at[pl.ds(pl.multiple_of(to_c * half, half), half), :], so.at[t], ss_so.at[i], rs_so.at[i], peer
            )
        )
    mine = pl.multiple_of(c * half, half)
    so[t] = so_own[pl.ds(mine, half), :]

    def mix_rows(at):
        return mo.at[:, pl.ds(pl.multiple_of(at * side, side), side), :]

    send(lambda: remote(mix_rows(t), mix_rows(t), ss_mc.at[0], rs_mc.at[0], c_peer))
    t_x = (1 - x) * CORES + c
    for fs in range(2 * Z):
        ref = mo.at[fs, pl.ds(pl.multiple_of(t_x * side, side), side), :]
        remote(ref, ref, ss_mx.at[fs], rs_mx.at[fs], me).wait_recv()
    send(lambda: remote(mix_rows(t_x), mix_rows(t_x), ss_mc.at[1], rs_mc.at[1], c_peer))
    relay_ff((FG, FU))
    for i, peer in enumerate(tp_peers):
        ref = so.at[peer[1]]
        remote(ref, ref, ss_so.at[i], rs_so.at[i], me).wait_recv()
    for i, at in enumerate((x * CORES + 1 - c, (1 - x) * CORES + 1 - c)):
        ref = mix_rows(at)
        remote(ref, ref, ss_mc.at[i], rs_mc.at[i], me).wait_recv()

    @pl.loop(0, 2 * Z)
    def _(fs):
        cols = pl.ds(pl.multiple_of(fs * part, part), part)
        acc = residual_scale * tok[pl.ds(mine, half), cols].astype(jnp.float32)
        for i in range(2 * CORES):
            acc += dotf(so[i], mo[fs, i * side : (i + 1) * side, :])
        yb[:, cols] = acc

    own0 = zi * rows
    strip = 32

    @pl.loop(0, half // strip)
    def _(i):
        at = pl.multiple_of(i * strip, strip)
        v = yb[pl.ds(at, strip), :]
        mean = jnp.sum(v, axis=1, keepdims=True) / d
        spread = jnp.sum(v * v, axis=1, keepdims=True) / d - mean * mean
        fn[pl.ds(pl.multiple_of(own0 + mine + at, strip), strip), :] = (
            (v - mean) * lax.rsqrt(spread + norm_eps) * gain1[...]
        ).astype(jnp.bfloat16)

    tp_n = TOKEN_PIECES

    def token_rows(zz, cc, xx, p):
        n = quarter // tp_n
        at = zz * rows + cc * half + xx * quarter + p * n
        return fn.at[pl.ds(pl.multiple_of(at, n), n), :]

    def token_send(ref, i, peer):
        send(lambda: remote(ref(), ref(), ss_t.at[i], rs_t.at[i], peer))

    def token_wait(ref, i):
        remote(ref, ref, ss_t.at[i], rs_t.at[i], me).wait_recv()

    z_pair = z_peer(far(1))
    for p in range(tp_n):
        token_send(lambda p=p: token_rows(zi, c, x, p), 1 + p, z_pair)

    def own_half(cc):
        return fn.at[pl.ds(pl.multiple_of(own0 + cc * half, half), half), :]

    token_send(lambda: own_half(c), 0, c_peer)
    to_middle(DOWN, early)
    relay_ff((FG + 1, FU + 1))

    def ff(j, base, tiles):
        n = 512

        @pl.loop(0, tiles)
        def _(i):
            at = pl.ds(pl.multiple_of(base + i * n, n), n)
            a = fn[at, :]
            row = lax.broadcasted_iota(jnp.int32, (n, cw), 0) % SEQ
            cols = pl.ds(pl.multiple_of(offset(z) + j * cw, LANES), cw)

            def conv(w, taps):
                p = dotf(a, w[j])
                one = jnp.where(row >= 1, pltpu.roll(p, 1, 0), 0.0)
                two = jnp.where(row >= 2, pltpu.roll(p, 2, 0), 0.0)
                return taps[0:1, cols] * two + taps[1:2, cols] * one + taps[2:3, cols] * p

            gate = conv(wg, taps_g)
            res = jax.nn.silu(gate) * conv(wu, taps_u)
            lane = lax.broadcasted_iota(jnp.int32, (n, cw), 1) + j * cw
            mine_too = lane < shift + middle(z) * (window - shift)
            h[j, at, :] = jnp.where(mine_too, res, 0.0).astype(jnp.bfloat16)

    other0 = (1 - zi) * rows

    def down_pass(hops, when, kinds=DOWN):
        for kind in kinds:
            for k in hops:
                arrive(kind, 2 * far(k) + y, when)
                pass_y(kind, far(k), when)

    def pass_first(role, kinds=DOWN):
        down_pass((2, 3), late & role, kinds)
        down_pass((1,), early & role, kinds)

    def pass_second():
        for kind in DOWN:
            own_y(kind, late & inner)
        down_pass((1,), late)
        down_pass((2, 3), early)

    def down_ready(b):
        for kind in DOWN:
            for i in (0, 1):
                arrive(kind, 2 * (2 * (x if b else 1 - x) + i) + 1 - y)

    token_wait(own_half(1 - c), 0)
    settle((FG, FU))
    ff(0, own0, rows // 512)
    relay_ff((FG + 2, FU + 2))
    for kind in DOWN:
        own_y(kind, early | outer)
    for p in range(tp_n):
        token_wait(token_rows(1 - zi, c, x, p), 1 + p)
        token_send(lambda p=p: token_rows(1 - zi, c, x, p), 1 + tp_n + p, x_peer)
        token_send(lambda p=p: token_rows(1 - zi, c, x, p), 1 + 2 * tp_n + p, c_peer)
    to_middle(DOWN, late)
    settle((FG + 1, FU + 1))
    ff(1, own0, rows // 512)
    to_ends(DOWN, when=early)
    settle((FG + 2, FU + 2))
    ff(2, own0, rows // 512)
    to_ends(DOWN, when=late)
    for p in range(tp_n):
        token_wait(token_rows(1 - zi, c, 1 - x, p), 1 + tp_n + p)
        token_send(lambda p=p: token_rows(1 - zi, c, 1 - x, p), 1 + 3 * tp_n + p, c_peer)
    for p in range(tp_n):
        token_wait(token_rows(1 - zi, 1 - c, x, p), 1 + 2 * tp_n + p)
        token_wait(token_rows(1 - zi, 1 - c, 1 - x, p), 1 + 3 * tp_n + p)

    pass_first(inner)
    for j in range(CHUNKS):
        ff(j, other0, rows // 512)
        pass_first(outer, (DOWN[j],))
    pass_second()
    for kind in DOWN:
        own_wait(kind)
    def rr(q):
        return pl.ds(pl.multiple_of((other0 + q * piece) % (2 * rows), piece), piece)

    def product(q, zf, yy):
        w = wd.at[2 * zf + yy]
        acc = dotf(h[0, rr(q), :], w[0:cw, :])
        for j in range(1, CHUNKS):
            acc += dotf(h[j, rr(q), :], w[j * cw : (j + 1) * cw, :])
        return acc

    def core_copy(b, q):
        return remote(s1.at[b, q], r1.at[b, q], ss_c.at[b, q], rs_c.at[b, q], c_peer)

    def x_copy(q):
        return remote(s2.at[q], r2.at[q], ss_x.at[q], rs_x.at[q], x_peer)

    def z_copy(q):
        return remote(s3.at[q], r3.at[q], ss_e.at[q], rs_e.at[q], z_pair)

    half_pieces = PIECES // 2

    def reduce_core(b):
        xo = x if b else 1 - x

        @pl.loop(0, PIECES)
        def _(q):
            for yy in (0, 1):
                s1[b, q, :, yy * part : (yy + 1) * part] = product(q, 2 * xo + 1 - c, yy).astype(jnp.bfloat16)
            core_copy(b, q).start()

        @pl.loop(0, PIECES)
        def _(q):
            own = [product(q, 2 * xo + c, yy) for yy in (0, 1)]
            core_copy(b, q).wait_recv()
            first, second = [
                own[yy] + r1[b, q, :, yy * part : (yy + 1) * part].astype(jnp.float32) for yy in (0, 1)
            ]

            if b:
                keep[q, :, :part] = first
                keep[q, :, part:] = second
            else:
                s2[q] = first.astype(jnp.bfloat16)
                x_copy(q).start()

            @pl.when(q < half_pieces)
            def _():
                s3[half_pieces * b + q] = second.astype(jnp.bfloat16)
                z_copy(half_pieces * b + q).start()

            if not b:

                @pl.when(q >= half_pieces)
                def _():
                    keep_x[q - half_pieces] = second

    down_ready(0)
    reduce_core(0)
    down_ready(1)
    reduce_core(1)

    @pl.loop(0, half_pieces)
    def _(q):
        z_copy(q).wait_recv()
        s2[PIECES + q] = (keep_x[q] + r3[q].astype(jnp.float32)).astype(jnp.bfloat16)
        x_copy(PIECES + q).start()

    @pl.loop(0, half_pieces)
    def _(q):
        x_copy(q).wait_recv()
        s3[2 * half_pieces + q] = (keep[q, :, :part] + r2[q].astype(jnp.float32)).astype(jnp.bfloat16)
        z_copy(2 * half_pieces + q).start()

    out_cols = pl.ds(pl.multiple_of(t * width2, width2), width2)

    @pl.loop(0, PIECES // 2)
    def _(q):
        own_piece = q + half_pieces
        z_copy(half_pieces + q).wait_recv()
        x_copy(own_piece).wait_recv()
        z_copy(2 * half_pieces + q).wait_recv()
        x_copy(PIECES + q).wait_recv()
        first = r2[own_piece].astype(jnp.float32) + r3[2 * half_pieces + q].astype(jnp.float32)
        second = r2[PIECES + q].astype(jnp.float32) + r3[half_pieces + q].astype(jnp.float32)
        v = keep[own_piece] + jnp.concatenate([first, second], axis=1)
        v += residual_scale * fn[rr(q + PIECES // 2), out_cols].astype(jnp.float32)
        keep[q + PIECES // 2] = v
        st[1, :, pl.ds(pl.multiple_of(q * piece, piece), piece)] = stat_rows(
            jnp.sum(v, axis=1, keepdims=True), jnp.sum(v * v, axis=1, keepdims=True)
        )

    stats_out(1)
    stats_in(1)

    @pl.loop(0, rows // LANES)
    def _(n):
        at = pl.ds(pl.multiple_of(n * LANES, LANES), LANES)
        mean, scale = moments(1, at, d)
        mean = jnp.concatenate([mean] * (width2 // LANES), axis=1)
        scale = jnp.concatenate([scale] * (width2 // LANES), axis=1)
        per = piece // LANES
        v = keep[PIECES // 2 + n // per, pl.ds(pl.multiple_of((n % per) * LANES, LANES), LANES), :]
        out[at, :] = ((v - mean) * scale * gain2[:, out_cols]).astype(jnp.bfloat16)

    @pl.loop(0, PIECES)
    def _(q):
        core_copy(0, q).wait_send()
        core_copy(1, q).wait_send()

    @pl.loop(0, 3 * half_pieces)
    def _(q):
        x_copy(q).wait_send()
        z_copy(q).wait_send()

    for end in drain:
        end()


def per_device_small(
    tokens,
    w_gate_side,
    w_value_side,
    spatial_gain,
    w_spatial,
    spatial_bias,
    w_mixer_out,
    first_gain,
    w_ff_gate,
    w_ff_up,
    conv_gate_taps,
    conv_up_taps,
    w_ff_down,
    second_gain,
):
    rows, d = tokens.shape
    side = w_gate_side.shape[1]
    n_fs = lax.axis_size("fs")
    part = d // n_fs
    hid = w_ff_gate.shape[1]
    window = -(-hid // (2 * LANES)) * LANES
    cw = window // CHUNKS
    piece = 2 * rows // PIECES
    width2 = d // lax.axis_size("tp")
    bf, f32 = jnp.bfloat16, jnp.float32
    vmem, dma = pltpu.VMEM, pltpu.SemaphoreType.DMA
    anywhere = pl.BlockSpec(memory_space=pl.ANY)
    local = pl.BlockSpec(memory_space=pltpu.VMEM)
    return pl.pallas_call(
        layer_kernel,
        out_shape=jax.ShapeDtypeStruct((rows, width2), bf),
        in_specs=[anywhere] * 14,
        out_specs=local,
        scratch_shapes=[
            vmem((1, side), f32),
            vmem(w_spatial.shape, bf),
            vmem(spatial_bias.shape, f32),
            vmem((1, d), f32),
            vmem(conv_gate_taps.shape, f32),
            vmem(conv_up_taps.shape, f32),
            vmem((1, d), f32),
            vmem((rows, d), bf),
            vmem((d, side), bf),
            vmem((d, side), bf),
            vmem((n_fs, side * 2 * CORES, part), bf),
            vmem((CHUNKS, d, cw), bf),
            vmem((CHUNKS, d, cw), bf),
            vmem((n_fs, window, part), bf),
            vmem((rows, side), f32),
            vmem((rows, side), f32),
            vmem((rows, side), bf),
            vmem((2 * CORES, rows // 2, side), bf),
            vmem((rows // 2, d), f32),
            vmem((2 * rows, d), bf),
            vmem((CHUNKS, 2 * rows, cw), bf),
            vmem((2, PIECES, piece, width2), bf),
            vmem((2, PIECES, piece, width2), bf),
            vmem((3 * PIECES // 2, piece, part), bf),
            vmem((3 * PIECES // 2, piece, part), bf),
            vmem((3 * PIECES // 2, piece, part), bf),
            vmem((3 * PIECES // 2, piece, part), bf),
            vmem((PIECES, piece, width2), f32),
            vmem((PIECES // 2, piece, part), f32),
            vmem((SPAN, side), f32),
            vmem((2, 8, rows), f32),
            vmem((2, 3, 8, rows), f32),
            dma((KINDS, n_fs)),
            dma((KINDS, Z + 1)),
            dma((KINDS, Z)),
            dma((n_fs,)),
            dma((n_fs,)),
            dma((2,)),
            dma((2,)),
            dma((1 + KINDS + 7,)),
            dma((2, 3)),
            dma((2, 3)),
            dma((3,)),
            dma((3,)),
            dma((1 + 4 * TOKEN_PIECES,)),
            dma((1 + 4 * TOKEN_PIECES,)),
            dma((2, PIECES)),
            dma((2, PIECES)),
            dma((3 * PIECES // 2,)),
            dma((3 * PIECES // 2,)),
            dma((3 * PIECES // 2,)),
            dma((3 * PIECES // 2,)),
        ],
        compiler_params=pltpu.CompilerParams(
            collective_id=0, has_side_effects=True, vmem_limit_bytes=VMEM_BYTES
        ),
        name="layer",
    )(
        tokens,
        w_gate_side,
        w_value_side,
        spatial_gain.reshape(1, -1),
        w_spatial,
        spatial_bias,
        w_mixer_out,
        first_gain.reshape(1, -1),
        w_ff_gate,
        w_ff_up,
        conv_gate_taps,
        conv_up_taps,
        w_ff_down,
        second_gain.reshape(1, -1),
    )


def solution(mesh):
    small = mesh.shape["fs"] == 2 * Z and mesh.shape["tp"] == 2 * CORES
    body = per_device_small if small else per_device
    return jax.shard_map(
        body,
        mesh=mesh,
        in_specs=(
            P("fs", None),
            P("fs", "tp"),
            P("fs", "tp"),
            P("tp"),
            P("tp", None, None),
            P("tp", None),
            P("tp", "fs"),
            P(),
            P("fs", "tp"),
            P("fs", "tp"),
            P(None, "tp"),
            P(None, "tp"),
            P("tp", "fs"),
            P(),
        ),
        out_specs=P("fs", "tp"),
        check_vma=False,
    )
```

```python
import jax
import jax.numpy as jnp
from jax import lax
from jax.experimental import pallas as pl
from jax.experimental.pallas import tpu as pltpu
from jax.sharding import PartitionSpec as P

GROUP_DIM = 64
SPAN = 128
SEQ = 256
Z = 4
CORES = 2

residual_scale = 2.0**0.25
norm_eps = 1e-05


def fs_pairs(n_fs, dz, dy):
    n_y = n_fs // Z
    pairs = []
    for index in range(n_fs):
        z, y = index // n_y, index % n_y
        pairs.append((index, (z + dz) % Z * n_y + (y + dy) % n_y))
    return pairs


def tp_pairs(n_tp, dx, dc):
    n_x = n_tp // CORES
    pairs = []
    for index in range(n_tp):
        x, c = index // CORES, index % CORES
        pairs.append((index, (x + dx) % n_x * CORES + (c + dc) % CORES))
    return pairs


def move_fs(value, dz, dy):
    return lax.ppermute(value, "fs", fs_pairs(lax.axis_size("fs"), dz, dy))


def move_tp(value, dx, dc):
    return lax.ppermute(value, "tp", tp_pairs(lax.axis_size("tp"), dx, dc))


def y_blocks(own):
    n_y = lax.axis_size("fs") // Z
    y = lax.axis_index("fs") % n_y
    pieces = [own]
    for step in range(1, n_y):
        pieces.append(move_fs(pieces[-1], 0, 1))
    return [lax.select_n((y - at) % n_y, *pieces) if n_y > 2 else lax.select_n((y - at) % n_y == 1, *pieces) for at in range(n_y)]


def z_ring(own):
    right = move_fs(own, 1, 0)
    left = move_fs(own, -1, 0)
    far = move_fs(right, 1, 0)
    return [own, left, far, right]


def row_norm(values, gain):
    width = values.shape[1]
    mean = jnp.sum(values, axis=1, keepdims=True) / width
    spread = jnp.sum(values * values, axis=1, keepdims=True) / width - mean * mean
    return (values - mean) * lax.rsqrt(spread + norm_eps) * gain


def scatter_rows(part):
    n_tp = lax.axis_size("tp")
    n_x = n_tp // CORES
    tp = lax.axis_index("tp")
    x, c = tp // CORES, tp % CORES
    rows, cols = part.shape
    blocks = part.astype(jnp.bfloat16).reshape(n_x, CORES, rows // n_tp, cols)
    mine = lax.dynamic_index_in_dim(blocks, c, 1, keepdims=False)
    other = lax.dynamic_index_in_dim(blocks, 1 - c, 1, keepdims=False)
    pair = mine.astype(jnp.float32) + move_tp(other, 0, 1).astype(jnp.float32)
    total = lax.dynamic_index_in_dim(pair, x, 0, keepdims=False)
    for dx in range(1, n_x):
        away = lax.dynamic_index_in_dim(pair, (x + dx) % n_x, 0, keepdims=False)
        total = total + move_tp(away.astype(jnp.bfloat16), dx, 0).astype(jnp.float32)
    return total


def gather_rows(own):
    n_tp = lax.axis_size("tp")
    n_x = n_tp // CORES
    tp = lax.axis_index("tp")
    x, c = tp // CORES, tp % CORES
    column = [own]
    for dx in range(1, n_x):
        column.append(move_tp(own, dx, 0))
    column_abs = [
        lax.select_n((x - at) % n_x == 1, *column) if n_x == 2 else lax.select_n((x - at) % n_x, *column)
        for at in range(n_x)
    ]
    near = [move_tp(value, 0, 1) for value in column]
    near_abs = [
        lax.select_n((x - at) % n_x == 1, *near) if n_x == 2 else lax.select_n((x - at) % n_x, *near)
        for at in range(n_x)
    ]
    pieces = []
    for at in range(n_x):
        pieces.append(jnp.where(c == 0, column_abs[at], near_abs[at]))
        pieces.append(jnp.where(c == 0, near_abs[at], column_abs[at]))
    return jnp.concatenate(pieces, axis=0)


def rows_to_columns(own):
    n_tp = lax.axis_size("tp")
    n_x = n_tp // CORES
    tp = lax.axis_index("tp")
    x, c = tp // CORES, tp % CORES
    rows, cols = own.shape
    width = cols // n_tp
    result = jnp.zeros((n_tp * rows, width), own.dtype)
    for dx in range(n_x):
        for dc in range(CORES):
            to = (x + dx) % n_x * CORES + (c + dc) % CORES
            came = (x - dx) % n_x * CORES + (c - dc) % CORES
            block = lax.dynamic_slice_in_dim(own, to * width, width, 1)
            if dx or dc:
                block = move_tp(block, dx, dc)
            result = lax.dynamic_update_slice_in_dim(result, block, came * rows, 0)
    return result


def causal_taps(pre, taps):
    count = pre.shape[0] // SEQ
    blocks = pre.reshape(count, SEQ, pre.shape[1])
    padded = jnp.pad(blocks, ((0, 0), (2, 0), (0, 0)))
    result = padded[:, 0:SEQ] * taps[0] + padded[:, 1 : SEQ + 1] * taps[1] + padded[:, 2:] * taps[2]
    return result.reshape(pre.shape)


def mm(left, right):
    return jnp.dot(left, right, preferred_element_type=jnp.float32)


def split_norm(values, gain, width):
    sums = jnp.stack([jnp.sum(values, axis=1), jnp.sum(values * values, axis=1)])
    n_x = lax.axis_size("tp") // CORES
    total = sums
    for dx in range(n_x):
        for dc in range(CORES):
            if dx or dc:
                total = total + move_tp(sums, dx, dc)
    mean = total[0][:, None] / width
    spread = total[1][:, None] / width - mean * mean
    return (values - mean) * lax.rsqrt(spread + norm_eps) * gain


def per_device(
    tokens,
    w_gate_side,
    w_value_side,
    spatial_gain,
    w_spatial,
    spatial_bias,
    w_mixer_out,
    first_gain,
    w_ff_gate,
    w_ff_up,
    conv_gate_taps,
    conv_up_taps,
    w_ff_down,
    second_gain,
):
    rows, d = tokens.shape
    n_fs, n_tp = lax.axis_size("fs"), lax.axis_size("tp")
    n_y = n_fs // Z
    z = lax.axis_index("fs") // n_y
    tp = lax.axis_index("tp")
    shift = z * (d // Z)
    own_rows = rows // n_tp
    side = w_gate_side.shape[1]
    depth = w_gate_side.shape[0]

    near = y_blocks(jnp.concatenate([w_gate_side, w_value_side], axis=1))
    near_mix = y_blocks(w_mixer_out)
    sides = z_ring(jnp.concatenate(near, axis=0))
    mixes = z_ring(jnp.concatenate(near_mix, axis=1))
    gate_z = z_ring(w_ff_gate)
    gate_w = jnp.concatenate([b for s in gate_z for b in y_blocks(s)], axis=0)
    up_z = z_ring(w_ff_up)
    up_w = jnp.concatenate([b for s in up_z for b in y_blocks(s)], axis=0)
    down_z = z_ring(w_ff_down)
    down_w = [jnp.concatenate(y_blocks(s), axis=1) for s in down_z]

    tokens_rel = jnp.roll(tokens, -shift, axis=1)
    pre = mm(tokens_rel, jnp.concatenate(sides, axis=0))
    gate_act = jax.nn.gelu(pre[:, :side])
    value_norm = split_norm(
        jax.nn.gelu(pre[:, side:]), spatial_gain, side * n_tp
    ).astype(jnp.bfloat16)
    groups_dev = w_spatial.shape[0]
    blocks = value_norm.reshape(rows // SPAN, SPAN, groups_dev, GROUP_DIM)
    lower = jnp.tril(jnp.ones((SPAN, SPAN), jnp.bool_))
    causal_w = jnp.where(lower[None], w_spatial, jnp.zeros_like(w_spatial))
    mixed = jnp.einsum("gts,nsgc->ntgc", causal_w, blocks, preferred_element_type=jnp.float32)
    mixed = mixed + spatial_bias.T[None, :, :, None]
    spatial_out = (gate_act * mixed.reshape(rows, side)).astype(jnp.bfloat16)
    mixer_sum = scatter_rows(mm(spatial_out, jnp.concatenate(mixes, axis=1)))
    own_tokens = lax.dynamic_slice_in_dim(tokens_rel, tp * own_rows, own_rows, 0)
    first_own = row_norm(
        residual_scale * own_tokens.astype(jnp.float32) + mixer_sum, jnp.roll(first_gain, -shift)
    ).astype(jnp.bfloat16)
    first_whole = gather_rows(first_own)

    ff_gate = causal_taps(mm(first_whole, gate_w), conv_gate_taps)
    ff_up = causal_taps(mm(first_whole, up_w), conv_up_taps)
    ff_hidden = (jax.nn.silu(ff_gate) * ff_up).astype(jnp.bfloat16)
    ff_sum = jnp.concatenate([scatter_rows(mm(ff_hidden, piece)) for piece in down_w], axis=1)
    out_rel = row_norm(
        residual_scale * first_own.astype(jnp.float32) + ff_sum, jnp.roll(second_gain, -shift)
    ).astype(jnp.bfloat16)
    return rows_to_columns(jnp.roll(out_rel, shift, axis=1))


LANES = 128
CHUNKS = 3
SG, SV, MO, FG, FU, FD = 0, 1, 2, 3, 3 + CHUNKS, 3 + 2 * CHUNKS
KINDS = 3 + 3 * CHUNKS
DOWN = tuple(range(FD, KINDS))
PIECES = 4
TOKEN_PIECES = 4
MESH = pl.DeviceIdType.MESH
VMEM_BYTES = 67043328


def to_rows(column, rows):
    n = column.shape[0]
    return jnp.transpose(jnp.broadcast_to(column, (n, LANES)))[:rows]


def to_columns(row):
    return jnp.transpose(jnp.broadcast_to(row, (LANES, LANES)))


def stat_rows(first, second):
    a, b = to_rows(first, 8), to_rows(second, 8)
    at = lax.broadcasted_iota(jnp.int32, a.shape, 0)
    return jnp.where(at == 0, a, jnp.where(at == 1, b, 0.0))


def dotf(a, b):
    return jnp.dot(a, b, preferred_element_type=jnp.float32)


def layer_kernel(
    tokens,
    wgs,
    wvs,
    sgain_in,
    wsp_in,
    sbias_in,
    wmix,
    gain1_in,
    wgate,
    wup,
    taps_g_in,
    taps_u_in,
    wdown,
    gain2_in,
    out,
    sgain,
    wsp,
    sbias,
    gain1,
    taps_g,
    taps_u,
    gain2,
    tok,
    swg,
    swv,
    mo,
    wg,
    wu,
    wd,
    ga,
    va,
    so_own,
    so,
    yb,
    fn,
    h,
    s1,
    r1,
    s2,
    r2,
    s3,
    r3,
    keep,
    keep_x,
    biasf,
    st,
    rst,
    rs_w,
    ss_z,
    ss_y,
    ss_mx,
    rs_mx,
    ss_mc,
    rs_mc,
    lsem,
    ss_st,
    rs_st,
    ss_so,
    rs_so,
    ss_t,
    rs_t,
    ss_c,
    rs_c,
    ss_x,
    rs_x,
    ss_e,
    rs_e,
    osem,
):
    f, t = lax.axis_index("fs"), lax.axis_index("tp")
    z, y = f // 2, f % 2
    x, c = t // CORES, t % CORES
    zi = z % 2
    rows, d = tok.shape
    side = swg.shape[1]
    part = d // (2 * Z)
    hid = wgate.shape[1]
    window = wd.shape[1]
    cw = window // CHUNKS
    shift = hid - window
    half, quarter = rows // 2, rows // 4
    width2 = d // 4
    piece = 2 * rows // PIECES

    def far(k):
        if k == 1:
            return z + 1 - 2 * (z % 2)
        return (z + 2) % Z if k == 2 else Z - 1 - z

    def middle(at):
        return ((at + 1) // 2) % 2

    def offset(at):
        return pl.multiple_of(middle(at) * shift, LANES)

    me = (f, t)
    y_peer = (2 * z + 1 - y, t)
    x_peer = (f, (1 - x) * CORES + c)
    c_peer = (f, x * CORES + 1 - c)
    xc_peer = (f, (1 - x) * CORES + 1 - c)

    def z_peer(at):
        return (2 * at + y, t)

    tp_peers = (c_peer, x_peer, xc_peer)
    barrier = pltpu.get_barrier_semaphore()
    greeted = (y_peer,) + tp_peers + tuple(z_peer(far(k)) for k in (1, 2, 3))
    for peer in greeted:
        pl.semaphore_signal(barrier, inc=1, device_id=peer, device_id_type=MESH)
    pl.semaphore_wait(barrier, len(greeted))

    def remote(src, dst, ss, rs, to):
        return pltpu.make_async_remote_copy(
            src_ref=src, dst_ref=dst, send_sem=ss, recv_sem=rs, device_id=to, device_id_type=MESH
        )

    late = z // 2 == x
    early = z // 2 != x
    outer = middle(z) == 0
    inner = middle(z) == 1

    def cut(kind):
        return min(cw, shift - ((kind - FG) % CHUNKS) * cw)

    def varies(kind):
        return kind >= FG and cut(kind) != cw

    def source(kind, off, narrow=False):
        if kind == SG:
            return wgs
        if kind == SV:
            return wvs
        if kind == MO:
            return wmix
        at = pl.multiple_of(off + ((kind - FG) % CHUNKS) * cw, LANES)
        cols = pl.ds(at, cut(kind) if narrow else cw)
        if kind >= FD:
            return wdown.at[cols, :]
        return (wgate if kind < FU else wup).at[:, cols]

    def slot(kind, fsrc, narrow=False):
        at = pl.ds(pl.multiple_of(fsrc * part, part), part)
        if kind == SG:
            return swg.at[at, :]
        if kind == SV:
            return swv.at[at, :]
        if kind == MO:
            return mo.at[fsrc, pl.ds(pl.multiple_of(t * side, side), side), :]
        if kind >= FD:
            return wd.at[fsrc, pl.ds((kind - FD) * cw, cut(kind) if narrow else cw), :]
        return (wg if kind < FU else wu).at[(kind - FG) % CHUNKS, at, pl.ds(0, cut(kind) if narrow else cw)]

    drain = []

    def guard(when, role):
        return role if when is None else when & role

    def run(when, act):
        if when is None:
            act()
        else:
            pl.when(when)(act)

    def send(make, when=None):
        run(when, lambda: make().start())
        drain.append(lambda: run(when, lambda: make().wait_send()))

    def by_role(kind, act, when=None):
        if varies(kind):
            act(False, guard(when, inner))
            act(True, guard(when, outer))
        else:
            act(False, when)

    def arrive(kind, fsrc, when=None):
        def act(narrow, on):
            ref = slot(kind, fsrc, narrow)
            run(on, lambda: remote(ref, ref, ss_y.at[kind, 0], rs_w.at[kind, fsrc], me).wait_recv())

        by_role(kind, act, when)

    def own_local(kind, narrow):
        return pltpu.make_async_copy(source(kind, offset(z), narrow), slot(kind, f, narrow), lsem.at[1 + kind])

    def own_start(kind):
        by_role(kind, lambda narrow, on: run(on, lambda: own_local(kind, narrow).start()))

    def own_wait(kind, when=None):
        by_role(kind, lambda narrow, on: run(on, lambda: own_local(kind, narrow).wait()), when)

    def own_y(kind, when=None):
        by_role(
            kind,
            lambda narrow, on: send(
                lambda: remote(
                    source(kind, offset(z), narrow), slot(kind, f, narrow), ss_y.at[kind, z], rs_w.at[kind, f], y_peer
                ),
                on,
            ),
            when,
        )

    def own_z(kind, k, when, narrow):
        to = far(k)
        narrow = narrow and varies(kind)
        send(
            lambda: remote(
                source(kind, offset(to), narrow), slot(kind, f, narrow), ss_z.at[kind, k], rs_w.at[kind, f], z_peer(to)
            ),
            when,
        )

    def pass_y(kind, zs, when=None):
        fs = 2 * zs + y

        def act(narrow, on):
            send(
                lambda: remote(
                    slot(kind, fs, narrow), slot(kind, fs, narrow), ss_y.at[kind, zs], rs_w.at[kind, fs], y_peer
                ),
                on,
            )

        by_role(kind, act, when)

    def line_own(kind):
        send(lambda: remote(source(kind, 0), slot(kind, f), ss_z.at[kind, Z], rs_w.at[kind, f], z_peer(z + 1)), z < Z - 1)
        send(lambda: remote(source(kind, 0), slot(kind, f), ss_z.at[kind, z], rs_w.at[kind, f], z_peer(z - 1)), z > 0)

    def line_step(kinds, dist, also=None):
        for sign in (-1, 1):
            zs = z + sign * dist
            ok = (zs >= 0) & (zs < Z)
            on = ok & (z < Z - 1) if sign < 0 else ok & (z > 0)
            to = z - sign
            fs = 2 * zs + y
            for kind in kinds:

                def came(kind=kind, fs=fs):
                    arrive(kind, fs)

                pl.when(ok)(came)
                send(
                    lambda kind=kind, fs=fs, zs=zs, to=to: remote(
                        slot(kind, fs), slot(kind, fs), ss_z.at[kind, zs], rs_w.at[kind, fs], z_peer(to)
                    ),
                    on,
                )
                pass_y(kind, zs, ok)
                if kind == MO and also is not None:
                    also(fs, ok)

    def mix_x(fs, when=None):
        send(lambda: remote(slot(MO, fs), slot(MO, fs), ss_mx.at[fs], rs_mx.at[fs], x_peer), when)

    def relay_ff(kinds):
        for k in (1, 2, 3):
            for kind in kinds:
                arrive(kind, 2 * far(k) + y)
                pass_y(kind, far(k))

    def settle(kinds):
        for kind in kinds:
            own_wait(kind)
            for zs in range(Z):
                arrive(kind, 2 * zs + 1 - y)

    load_tokens = pltpu.make_async_copy(tokens, tok, lsem.at[0])
    load_tokens.start()
    small = [
        pltpu.make_async_copy(src, dst, lsem.at[1 + KINDS + i])
        for i, (src, dst) in enumerate(
            (
                (sgain_in, sgain),
                (wsp_in, wsp),
                (sbias_in, sbias),
                (gain1_in, gain1),
                (taps_g_in, taps_g),
                (taps_u_in, taps_u),
                (gain2_in, gain2),
            )
        )
    ]
    for kind in (SG, SV, MO):
        line_own(kind)
        own_y(kind)
    for kind in range(KINDS):
        own_start(kind)
    send(lambda: remote(wmix, slot(MO, f), ss_mx.at[f], rs_mx.at[f], x_peer))
    for copy in small:
        copy.start()

    def to_middle(kinds, when=None):
        for kind in kinds:
            own_z(kind, 3, guard(when, inner), False)
            own_z(kind, 2, guard(when, outer), False)
            own_z(kind, 1, guard(when, outer), False)

    def to_ends(kinds, hops=(3, 2, 1), when=None):
        for kind in kinds:
            for k in hops:
                own_z(kind, k, guard(when, outer if k == 3 else inner), True)

    def mix_y_to_x(dist):
        for sign in (-1, 1) if dist else (1,):
            zs = z + sign * dist
            ok = (zs >= 0) & (zs < Z)
            fs = 2 * zs + 1 - y
            pl.when(ok)(lambda fs=fs: arrive(MO, fs))
            mix_x(fs, ok)

    @pl.when(outer)
    def _():
        wd[:, shift:, :] = jnp.zeros((2 * Z, window - shift, part), wd.dtype)
        for ref in (wg, wu):
            ref[CHUNKS - 1, :, cut(FU - 1) :] = jnp.zeros((d, window - shift), ref.dtype)

    line_step((SG, SV, MO), 1, mix_x)
    mix_y_to_x(0)
    line_step((SG, SV, MO), 2, mix_x)
    to_middle((FG, FU))
    mix_y_to_x(1)
    line_step((SG, SV, MO), 3, mix_x)
    to_ends((FG, FU))
    to_middle((FG + 1, FU + 1))
    to_ends((FG + 1, FU + 1))
    to_middle((FG + 2, FU + 2))
    to_ends((FG + 2, FU + 2))
    for chunk in range(CHUNKS):
        own_y(FG + chunk)
        own_y(FU + chunk)

    for copy in small:
        copy.wait()

    lane2 = lax.broadcasted_iota(jnp.int32, (SPAN, side), 1) // GROUP_DIM
    groups = wsp.shape[0]
    bias_all = jnp.zeros((SPAN, side), jnp.float32)
    for g in range(groups):
        column = to_columns(sbias[g : g + 1, :])
        bias_all = jnp.where(lane2 == g, jnp.concatenate([column] * (side // LANES), axis=1), bias_all)
    biasf[...] = bias_all

    load_tokens.wait()
    settle((SG, SV))

    tile = 256

    @pl.loop(0, rows // tile)
    def _(i):
        at = pl.ds(pl.multiple_of(i * tile, tile), tile)
        a = tok[at, :]
        ga[at, :] = jax.nn.gelu(dotf(a, swg[...]))
        v = jax.nn.gelu(dotf(a, swv[...]))
        va[at, :] = v
        st[0, :, at] = stat_rows(jnp.sum(v, axis=1, keepdims=True), jnp.sum(v * v, axis=1, keepdims=True))

    def stats_copy(n, i, peer):
        at = pl.ds((n - 1) * piece, piece) if n else pl.ds(0, rows)
        which = min(n, 1)
        return remote(st.at[which, :, at], rst.at[which, i, :, at], ss_st.at[n, i], rs_st.at[n, i], peer)

    def stats_out(n):
        for i, peer in enumerate(tp_peers):
            send(lambda i=i, peer=peer: stats_copy(n, i, peer))

    def stats_in(n):
        for i in range(3):
            stats_copy(n, i, me).wait_recv()

    def moments(n, at, width):
        total = st[n, :, at] + rst[n, 0, :, at] + rst[n, 1, :, at] + rst[n, 2, :, at]
        mean = total[0:1] / width
        spread = total[1:2] / width - mean * mean
        return to_columns(mean), to_columns(lax.rsqrt(spread + norm_eps))

    stats_out(0)
    own_wait(MO)
    mix_y_to_x(2)
    mix_y_to_x(3)
    stats_in(0)

    @pl.loop(0, rows // SPAN)
    def _(n):
        at = pl.ds(pl.multiple_of(n * SPAN, SPAN), SPAN)
        mean, scale = moments(0, at, side * 2 * CORES)
        mean = jnp.concatenate([mean] * (side // LANES), axis=1)
        scale = jnp.concatenate([scale] * (side // LANES), axis=1)
        vn = ((va[at, :] - mean) * scale * sgain[...]).astype(jnp.bfloat16)
        low = lax.broadcasted_iota(jnp.int32, (SPAN, SPAN), 0) >= lax.broadcasted_iota(jnp.int32, (SPAN, SPAN), 1)
        group = lax.broadcasted_iota(jnp.int32, (SPAN, side), 1) // GROUP_DIM
        mixed = jnp.zeros((SPAN, side), jnp.float32)
        for g in range(groups):
            w = jnp.where(low, wsp[g].astype(jnp.float32), 0.0).astype(jnp.bfloat16)
            mixed = jnp.where(group == g, dotf(w, vn), mixed)
        so_own[at, :] = (ga[at, :] * (mixed + biasf[...])).astype(jnp.bfloat16)

    for i, peer in enumerate(tp_peers):
        to_c = 1 - c if i != 1 else c
        send(
            lambda i=i, peer=peer, to_c=to_c: remote(
                so_own.at[pl.ds(pl.multiple_of(to_c * half, half), half), :], so.at[t], ss_so.at[i], rs_so.at[i], peer
            )
        )
    mine = pl.multiple_of(c * half, half)
    so[t] = so_own[pl.ds(mine, half), :]

    def mix_rows(at):
        return mo.at[:, pl.ds(pl.multiple_of(at * side, side), side), :]

    send(lambda: remote(mix_rows(t), mix_rows(t), ss_mc.at[0], rs_mc.at[0], c_peer))
    t_x = (1 - x) * CORES + c
    for fs in range(2 * Z):
        ref = mo.at[fs, pl.ds(pl.multiple_of(t_x * side, side), side), :]
        remote(ref, ref, ss_mx.at[fs], rs_mx.at[fs], me).wait_recv()
    send(lambda: remote(mix_rows(t_x), mix_rows(t_x), ss_mc.at[1], rs_mc.at[1], c_peer))
    relay_ff((FG, FU))
    for i, peer in enumerate(tp_peers):
        ref = so.at[peer[1]]
        remote(ref, ref, ss_so.at[i], rs_so.at[i], me).wait_recv()
    for i, at in enumerate((x * CORES + 1 - c, (1 - x) * CORES + 1 - c)):
        ref = mix_rows(at)
        remote(ref, ref, ss_mc.at[i], rs_mc.at[i], me).wait_recv()

    @pl.loop(0, 2 * Z)
    def _(fs):
        cols = pl.ds(pl.multiple_of(fs * part, part), part)
        acc = residual_scale * tok[pl.ds(mine, half), cols].astype(jnp.float32)
        for i in range(2 * CORES):
            acc += dotf(so[i], mo[fs, i * side : (i + 1) * side, :])
        yb[:, cols] = acc

    own0 = zi * rows
    strip = 32

    @pl.loop(0, half // strip)
    def _(i):
        at = pl.multiple_of(i * strip, strip)
        v = yb[pl.ds(at, strip), :]
        mean = jnp.sum(v, axis=1, keepdims=True) / d
        spread = jnp.sum(v * v, axis=1, keepdims=True) / d - mean * mean
        fn[pl.ds(pl.multiple_of(own0 + mine + at, strip), strip), :] = (
            (v - mean) * lax.rsqrt(spread + norm_eps) * gain1[...]
        ).astype(jnp.bfloat16)

    tp_n = TOKEN_PIECES

    def token_rows(zz, cc, xx, p):
        n = quarter // tp_n
        at = zz * rows + cc * half + xx * quarter + p * n
        return fn.at[pl.ds(pl.multiple_of(at, n), n), :]

    def token_send(ref, i, peer):
        send(lambda: remote(ref(), ref(), ss_t.at[i], rs_t.at[i], peer))

    def token_wait(ref, i):
        remote(ref, ref, ss_t.at[i], rs_t.at[i], me).wait_recv()

    z_pair = z_peer(far(1))
    for p in range(tp_n):
        token_send(lambda p=p: token_rows(zi, c, x, p), 1 + p, z_pair)

    def own_half(cc):
        return fn.at[pl.ds(pl.multiple_of(own0 + cc * half, half), half), :]

    token_send(lambda: own_half(c), 0, c_peer)
    to_middle(DOWN, early)
    relay_ff((FG + 1, FU + 1))

    def ff(j, base, tiles):
        n = 512

        @pl.loop(0, tiles)
        def _(i):
            at = pl.ds(pl.multiple_of(base + i * n, n), n)
            a = fn[at, :]
            row = lax.broadcasted_iota(jnp.int32, (n, cw), 0) % SEQ
            cols = pl.ds(pl.multiple_of(offset(z) + j * cw, LANES), cw)

            def conv(w, taps):
                p = dotf(a, w[j])
                one = jnp.where(row >= 1, pltpu.roll(p, 1, 0), 0.0)
                two = jnp.where(row >= 2, pltpu.roll(p, 2, 0), 0.0)
                return taps[0:1, cols] * two + taps[1:2, cols] * one + taps[2:3, cols] * p

            gate = conv(wg, taps_g)
            res = jax.nn.silu(gate) * conv(wu, taps_u)
            lane = lax.broadcasted_iota(jnp.int32, (n, cw), 1) + j * cw
            mine_too = lane < shift + middle(z) * (window - shift)
            h[j, at, :] = jnp.where(mine_too, res, 0.0).astype(jnp.bfloat16)

    other0 = (1 - zi) * rows

    def down_pass(hops, when, kinds=DOWN):
        for kind in kinds:
            for k in hops:
                arrive(kind, 2 * far(k) + y, when)
                pass_y(kind, far(k), when)

    def pass_outer(kind):
        down_pass((2, 3), late & outer, (kind,))
        down_pass((1,), early & outer, (kind,))

    def pass_second():
        for kind in DOWN:
            own_y(kind, late & inner)
        down_pass((1,), late)
        down_pass((2, 3), early & inner)

    def down_ready(b):
        for kind in DOWN:
            for i in (0, 1):
                arrive(kind, 2 * (2 * (x if b else 1 - x) + i) + 1 - y)

    token_wait(own_half(1 - c), 0)
    settle((FG, FU))
    ff(0, own0, rows // 512)
    relay_ff((FG + 2, FU + 2))
    for kind in DOWN:
        own_y(kind, early | outer)
    for p in range(tp_n):
        token_wait(token_rows(1 - zi, c, x, p), 1 + p)
        token_send(lambda p=p: token_rows(1 - zi, c, x, p), 1 + tp_n + p, x_peer)
        token_send(lambda p=p: token_rows(1 - zi, c, x, p), 1 + 2 * tp_n + p, c_peer)
    to_middle(DOWN, late)
    settle((FG + 1, FU + 1))
    ff(1, own0, rows // 512)
    to_ends(DOWN, when=early)
    settle((FG + 2, FU + 2))
    ff(2, own0, rows // 512)
    to_ends(DOWN, when=late)
    down_pass((2, 3), late & inner)
    for p in range(tp_n):
        token_wait(token_rows(1 - zi, c, 1 - x, p), 1 + tp_n + p)
        token_send(lambda p=p: token_rows(1 - zi, c, 1 - x, p), 1 + 3 * tp_n + p, c_peer)
    for p in range(tp_n):
        token_wait(token_rows(1 - zi, 1 - c, x, p), 1 + 2 * tp_n + p)
        token_wait(token_rows(1 - zi, 1 - c, 1 - x, p), 1 + 3 * tp_n + p)

    down_pass((1,), early & inner)
    for j in range(CHUNKS):
        pass_outer(DOWN[j])
        ff(j, other0, rows // 512)
    pass_second()
    for kind in DOWN:
        own_wait(kind)
    def rr(q):
        return pl.ds(pl.multiple_of((other0 + q * piece) % (2 * rows), piece), piece)

    def product(q, zf, yy):
        w = wd.at[2 * zf + yy]
        acc = dotf(h[0, rr(q), :], w[0:cw, :])
        for j in range(1, CHUNKS):
            acc += dotf(h[j, rr(q), :], w[j * cw : (j + 1) * cw, :])
        return acc

    def core_copy(b, q):
        return remote(s1.at[b, q], r1.at[b, q], ss_c.at[b, q], rs_c.at[b, q], c_peer)

    def x_copy(q):
        return remote(s2.at[q], r2.at[q], ss_x.at[q], rs_x.at[q], x_peer)

    def z_copy(q):
        return remote(s3.at[q], r3.at[q], ss_e.at[q], rs_e.at[q], z_pair)

    half_pieces = PIECES // 2

    def reduce_core(b):
        xo = x if b else 1 - x

        def theirs(q):
            for yy in (0, 1):
                s1[b, q, :, yy * part : (yy + 1) * part] = product(q, 2 * xo + 1 - c, yy).astype(jnp.bfloat16)
            core_copy(b, q).start()

        def ours(q):
            own = [product(q, 2 * xo + c, yy) for yy in (0, 1)]
            core_copy(b, q).wait_recv()
            first, second = [
                own[yy] + r1[b, q, :, yy * part : (yy + 1) * part].astype(jnp.float32) for yy in (0, 1)
            ]
            if b:
                keep[q, :, :part] = first
                keep[q, :, part:] = second
            else:
                s2[q] = first.astype(jnp.bfloat16)
                x_copy(q).start()

            @pl.when(q < half_pieces)
            def _():
                s3[half_pieces * b + q] = second.astype(jnp.bfloat16)
                z_copy(half_pieces * b + q).start()

            if not b:

                @pl.when(q >= half_pieces)
                def _():
                    keep_x[q - half_pieces] = second

        @pl.loop(0, PIECES + 1)
        def _(q):
            pl.when(q < PIECES)(lambda: theirs(q))
            pl.when(q > 0)(lambda: ours(q - 1))

    down_ready(0)
    reduce_core(0)
    down_pass((2, 3), early & outer)
    down_ready(1)
    reduce_core(1)

    @pl.loop(0, half_pieces)
    def _(q):
        z_copy(q).wait_recv()
        s2[PIECES + q] = (keep_x[q] + r3[q].astype(jnp.float32)).astype(jnp.bfloat16)
        x_copy(PIECES + q).start()

    @pl.loop(0, half_pieces)
    def _(q):
        x_copy(q).wait_recv()
        s3[2 * half_pieces + q] = (keep[q, :, :part] + r2[q].astype(jnp.float32)).astype(jnp.bfloat16)
        z_copy(2 * half_pieces + q).start()

    out_cols = pl.ds(pl.multiple_of(t * width2, width2), width2)

    def out_copy(q):
        return pltpu.make_async_copy(
            r1.at[0, q], out.at[pl.ds(q * piece, piece), :], osem.at[q]
        )

    for q in range(half_pieces):
        own_piece = q + half_pieces
        z_copy(half_pieces + q).wait_recv()
        x_copy(own_piece).wait_recv()
        z_copy(2 * half_pieces + q).wait_recv()
        x_copy(PIECES + q).wait_recv()
        first = r2[own_piece].astype(jnp.float32) + r3[2 * half_pieces + q].astype(jnp.float32)
        second = r2[PIECES + q].astype(jnp.float32) + r3[half_pieces + q].astype(jnp.float32)
        v = keep[own_piece] + jnp.concatenate([first, second], axis=1)
        v += residual_scale * fn[rr(own_piece), out_cols].astype(jnp.float32)
        keep[own_piece] = v
        st[1, :, q * piece : (q + 1) * piece] = stat_rows(
            jnp.sum(v, axis=1, keepdims=True), jnp.sum(v * v, axis=1, keepdims=True)
        )
        stats_out(1 + q)
        stats_in(1 + q)

        @pl.loop(0, piece // LANES)
        def _(n):
            at = pl.multiple_of(n * LANES, LANES)
            mean, scale = moments(1, pl.ds(pl.multiple_of(q * piece + at, LANES), LANES), d)
            mean = jnp.concatenate([mean] * (width2 // LANES), axis=1)
            scale = jnp.concatenate([scale] * (width2 // LANES), axis=1)
            block = pl.ds(at, LANES)
            r1[0, q, block, :] = ((keep[own_piece, block, :] - mean) * scale * gain2[:, out_cols]).astype(r1.dtype)

        out_copy(q).start()

    @pl.loop(0, PIECES)
    def _(q):
        core_copy(0, q).wait_send()
        core_copy(1, q).wait_send()

    @pl.loop(0, 3 * half_pieces)
    def _(q):
        x_copy(q).wait_send()
        z_copy(q).wait_send()

    for end in drain:
        end()
    for q in range(half_pieces):
        out_copy(q).wait()


def per_device_small(
    tokens,
    w_gate_side,
    w_value_side,
    spatial_gain,
    w_spatial,
    spatial_bias,
    w_mixer_out,
    first_gain,
    w_ff_gate,
    w_ff_up,
    conv_gate_taps,
    conv_up_taps,
    w_ff_down,
    second_gain,
):
    rows, d = tokens.shape
    side = w_gate_side.shape[1]
    n_fs = lax.axis_size("fs")
    part = d // n_fs
    hid = w_ff_gate.shape[1]
    window = -(-hid // (2 * LANES)) * LANES
    cw = window // CHUNKS
    piece = 2 * rows // PIECES
    width2 = d // lax.axis_size("tp")
    bf, f32 = jnp.bfloat16, jnp.float32
    vmem, dma = pltpu.VMEM, pltpu.SemaphoreType.DMA
    anywhere = pl.BlockSpec(memory_space=pl.ANY)
    return pl.pallas_call(
        layer_kernel,
        out_shape=jax.ShapeDtypeStruct((rows, width2), bf),
        in_specs=[anywhere] * 14,
        out_specs=anywhere,
        scratch_shapes=[
            vmem((1, side), f32),
            vmem(w_spatial.shape, bf),
            vmem(spatial_bias.shape, f32),
            vmem((1, d), f32),
            vmem(conv_gate_taps.shape, f32),
            vmem(conv_up_taps.shape, f32),
            vmem((1, d), f32),
            vmem((rows, d), bf),
            vmem((d, side), bf),
            vmem((d, side), bf),
            vmem((n_fs, side * 2 * CORES, part), bf),
            vmem((CHUNKS, d, cw), bf),
            vmem((CHUNKS, d, cw), bf),
            vmem((n_fs, window, part), bf),
            vmem((rows, side), f32),
            vmem((rows, side), f32),
            vmem((rows, side), bf),
            vmem((2 * CORES, rows // 2, side), bf),
            vmem((rows // 2, d), f32),
            vmem((2 * rows, d), bf),
            vmem((CHUNKS, 2 * rows, cw), bf),
            vmem((2, PIECES, piece, width2), bf),
            vmem((2, PIECES, piece, width2), bf),
            vmem((3 * PIECES // 2, piece, part), bf),
            vmem((3 * PIECES // 2, piece, part), bf),
            vmem((3 * PIECES // 2, piece, part), bf),
            vmem((3 * PIECES // 2, piece, part), bf),
            vmem((PIECES, piece, width2), f32),
            vmem((PIECES // 2, piece, part), f32),
            vmem((SPAN, side), f32),
            vmem((2, 8, rows), f32),
            vmem((2, 3, 8, rows), f32),
            dma((KINDS, n_fs)),
            dma((KINDS, Z + 1)),
            dma((KINDS, Z)),
            dma((n_fs,)),
            dma((n_fs,)),
            dma((2,)),
            dma((2,)),
            dma((1 + KINDS + 7,)),
            dma((1 + PIECES // 2, 3)),
            dma((1 + PIECES // 2, 3)),
            dma((3,)),
            dma((3,)),
            dma((1 + 4 * TOKEN_PIECES,)),
            dma((1 + 4 * TOKEN_PIECES,)),
            dma((2, PIECES)),
            dma((2, PIECES)),
            dma((3 * PIECES // 2,)),
            dma((3 * PIECES // 2,)),
            dma((3 * PIECES // 2,)),
            dma((3 * PIECES // 2,)),
            dma((PIECES // 2,)),
        ],
        compiler_params=pltpu.CompilerParams(
            collective_id=0, has_side_effects=True, vmem_limit_bytes=VMEM_BYTES
        ),
        name="layer",
    )(
        tokens,
        w_gate_side,
        w_value_side,
        spatial_gain.reshape(1, -1),
        w_spatial,
        spatial_bias,
        w_mixer_out,
        first_gain.reshape(1, -1),
        w_ff_gate,
        w_ff_up,
        conv_gate_taps,
        conv_up_taps,
        w_ff_down,
        second_gain.reshape(1, -1),
    )


def solution(mesh):
    small = mesh.shape["fs"] == 2 * Z and mesh.shape["tp"] == 2 * CORES
    body = per_device_small if small else per_device
    return jax.shard_map(
        body,
        mesh=mesh,
        in_specs=(
            P("fs", None),
            P("fs", "tp"),
            P("fs", "tp"),
            P("tp"),
            P("tp", None, None),
            P("tp", None),
            P("tp", "fs"),
            P(),
            P("fs", "tp"),
            P("fs", "tp"),
            P(None, "tp"),
            P(None, "tp"),
            P("tp", "fs"),
            P(),
        ),
        out_specs=P("fs", "tp"),
        check_vma=False,
    )
```
